256 devices in a mesh: ep: 64 (over z, y, core), tp: 4 (over x).
Axes of the slice: x: 4, y: 4, z: 8, core: 2. Of those that a mesh axis runs over, the one named last changes fastest.
Arguments:
- tokens: bfloat16 [1024, 2048], P('ep'), may hold values from -6 to 6
- norm_gain: bfloat16 [2048], replicated, may hold values from 0.099609375 to 1.8984375
- query_weight: bfloat16 [2048, 1024], P('ep', 'tp'), may hold values from -0.125 to 0.125
- key_weight: bfloat16 [2048, 1024], P('ep', 'tp'), may hold values from -0.125 to 0.125
- value_weight: bfloat16 [2048, 2048], P('ep', 'tp'), may hold values from -0.125 to 0.125
- outgate_weight: bfloat16 [2048, 2048], P('ep', 'tp'), may hold values from -0.125 to 0.125
- beta_weight: bfloat16 [2048, 16], replicated, may hold values from -0.125 to 0.125
- decay_weight: bfloat16 [2048, 16], replicated, may hold values from -0.125 to 0.125
- decay_rate: float32 [16], P('tp'), may hold values from 0.02 to 6
- decay_bias: float32 [16], P('tp'), may hold values from -3 to 3
- head_gain: bfloat16 [128], replicated, may hold values from 0.099609375 to 1.8984375
- recurrent: float32 [1024, 16, 128, 128], P('ep', 'tp'), may hold values from -3 to 3
- output_weight: bfloat16 [2048, 2048], P('tp', 'ep'), may hold values from -0.125 to 0.125
- ffn_gain: bfloat16 [2048], replicated, may hold values from 0.099609375 to 1.8984375
- routes: int32 [1024, 4], P('ep'), may hold values from 0 to 63, all different within a row; in each aligned block of 16 rows (0 to 15, 16 to 31, ...) at most 2 rows name the same one
- route_weight: float32 [1024, 4], P('ep'), may hold values from 0.1 to 1
- expert_gate: bfloat16 [64, 2048, 512], P('ep', None, 'tp'), may hold values from -0.125 to 0.125
- expert_up: bfloat16 [64, 2048, 512], P('ep', None, 'tp'), may hold values from -0.125 to 0.125
- expert_down: bfloat16 [64, 512, 2048], P('ep', 'tp'), may hold values from -0.25 to 0.25
- shared_gate: bfloat16 [2048, 512], P('ep', 'tp'), may hold values from -0.125 to 0.125
- shared_up: bfloat16 [2048, 512], P('ep', 'tp'), may hold values from -0.125 to 0.125
- shared_down: bfloat16 [512, 2048], P('tp', 'ep'), may hold values from -0.25 to 0.25
- branch_gate: bfloat16 [2048], replicated, may hold values from -0.125 to 0.125
Outputs:
- layer_out: bfloat16 [1024, 2048], P('ep')
- new_state: float32 [1024, 16, 128, 128], P('ep', 'tp')
The draws below stay inside these ranges and needn't reach their ends.
Inputs may be any that keep to these rules, and one draw needn't show every extreme that they name: `routes`: each row names 4 different experts. Among the rows of one aligned block of 16 rows no expert is named more than 2 times, and some block reaches it: one expert is named exactly 2 times there.
All inputs are finite; a program needn't handle non-finite values.
Results may differ from the reference program's by a relative error of at most 0.019.
Values may be sent and summed in bfloat16 or wider, within the bound.
No kernel may reach another device: no remote copies, remote signals or barrier semaphores. Data moves between devices by JAX's collectives and lax.ppermute only.
A program may use at most 64 MiB of HBM per device.

```python
import math
import jax
import jax.numpy as jnp
import numpy as np
from jax import lax

D = 2048
DK = 128
DV = 128
HK = 8
HV = 16
D_EXPERT = 512
D_SHARED = 512
TOPK = 4
SEQ_DEV = 16
SEQS = 1024
EXPERTS = 64
CAP = 2
N_EP = 64
N_TP = 4


def levels(stream_key, dims, shards, smallest, high):
    def one(position, blocks):
        draws = jax.random.uniform(jax.random.fold_in(jax.random.fold_in(stream_key, 6), position), (blocks,), jnp.float32, smallest / len(shards), high / len(shards))
        return jnp.repeat(jnp.exp(draws), dims[position] // blocks).reshape((-1,) + (1,) * (len(dims) - position - 1))

    level = one(*shards[0])
    for cut in shards[1:]:
        level = level * one(*cut)
    return level


def routed_block(stream_key, own, number, rows, number_of, top, most, slope):
    sequence = jax.random.permutation(stream_key, number_of)
    heavy_load, ordinary = shares(number_of, rows * top, most, slope, True), shares(number_of, rows * top, most, slope, False)
    places = jnp.arange(number_of)

    def named(sizes, turn):
        used = int((sizes > 0).sum())
        fixed = max(1, used // 4)
        shifted = fixed + (places - fixed + turn * (used - fixed)) % max(1, number_of - fixed)
        return jnp.zeros((number_of,), jnp.int32).at[sequence[jnp.where(places < fixed, places, shifted)]].set(jnp.asarray(sizes, jnp.int32))

    sizes = jnp.where(number % 4 == 0, named(heavy_load, number // 4), named(ordinary, number - number // 4 - 1))
    mixed = jax.random.permutation(jax.random.fold_in(own, 3), number_of)
    source_of, taker = mixed[0:number_of // 2 * 2:2], mixed[1:number_of // 2 * 2:2]
    margin = jnp.minimum(sizes[source_of] - 1, most - sizes[taker]) // 2
    margin = jnp.where((source_of == sequence[0]) | (taker == sequence[0]) | (sizes[taker] == 0), 0, jnp.maximum(margin, 0))
    shifted = jax.random.randint(jax.random.fold_in(own, 4), (number_of // 2,), 0, 1 << 20) % (margin + 1)
    sizes = sizes.at[source_of].add(-shifted).at[taker].add(shifted)
    items = jnp.searchsorted(jnp.cumsum(sizes), jnp.arange(rows * top), side="right").astype(jnp.int32)
    table = items.reshape(top, rows).T
    table = table[jax.random.permutation(jax.random.fold_in(own, 1), rows)]
    turn = jax.random.randint(jax.random.fold_in(own, 2), (rows, 1), 0, top)
    return jnp.take_along_axis(table, (jnp.arange(top)[None, :] + turn) % top, axis=1)


def shares(count, total, most, lean, full):
    loads = [(1 << 20) // math.isqrt(standing ** lean) + 1 for standing in range(1, count + 1)]
    largest = most if full else min(most, max(-(-total // count), total * loads[0] // sum(loads)))
    least = 1 if total - largest >= count - 1 else 0
    given, rest = [largest] + [least] * (count - 1), total - largest - least * (count - 1)
    while rest > 0:
        free = [i for i in range(1, count) if given[i] < largest] or [i for i in range(1, count) if given[i] < most]
        pool, left = sum([loads[i] for i in free]), rest
        for i in free:
            extra = min(most - given[i], max(1, left * loads[i] // pool), rest)
            given[i] = given[i] + extra
            rest = rest - extra
    return np.array(given)


def noise(stream_key, extent, deviation, reach, pieces=(), held_as=jnp.bfloat16):
    values = jax.random.normal(stream_key, extent, jnp.float32) * deviation
    if len(pieces) > 0:
        values = levels(stream_key, extent, pieces, -0.22, 0.18) * values
    return jnp.clip(values, min=-reach, max=reach).astype(held_as)


def setup_inputs(seed: int = 0) -> dict:
    key_of = jax.random.split(jax.random.key(seed), 24)
    tokens = noise(key_of[0], (SEQS, D), 1.0, 6.0, ((0, 64),))
    norm_gain = jnp.clip(1.0 + 0.18 * jax.random.normal(key_of[1], (D,), jnp.float32), 0.099609375, 1.8984375).astype(jnp.bfloat16)
    query_weight = noise(key_of[2], (D, HK * DK), D ** -0.5, 0.125, ((0, 64), (1, 4)))
    key_weight = noise(key_of[3], (D, HK * DK), D ** -0.5, 0.125, ((0, 64), (1, 4)))
    value_weight = noise(key_of[4], (D, HV * DV), D ** -0.5, 0.125, ((0, 64), (1, 4)))
    outgate_weight = noise(key_of[5], (D, HV * DV), D ** -0.5, 0.125, ((0, 64), (1, 4)))
    beta_weight = noise(key_of[6], (D, HV), D ** -0.5, 0.125)
    decay_weight = noise(key_of[7], (D, HV), D ** -0.5, 0.125)
    decay_rate = jnp.clip(jnp.exp(math.log(6.0) - 5.7037825 * jax.random.uniform(key_of[8], (HV,), jnp.float32) ** levels(key_of[8], (HV,), ((0, 4),), -0.2, 0.2)), 0.02, 6.0)
    decay_bias = noise(key_of[9], (HV,), 1.0, 3.0, ((0, 4),), jnp.float32)
    head_gain = jnp.clip(1.0 + 0.18 * jax.random.normal(key_of[10], (DV,), jnp.float32), 0.099609375, 1.8984375).astype(jnp.bfloat16)
    recurrent = noise(key_of[11], (SEQS, HV, DK, DV), 0.5, 3.0, ((0, 64), (1, 4)), jnp.float32)
    output_weight = noise(key_of[12], (HV * DV, D), (HV * DV) ** -0.5, 0.125, ((0, 4), (1, 64)))
    ffn_gain = jnp.clip(1.0 + 0.18 * jax.random.normal(key_of[13], (D,), jnp.float32), 0.099609375, 1.8984375).astype(jnp.bfloat16)
    routes_keys = jax.random.split(jax.random.fold_in(key_of[14], 1), SEQS // SEQ_DEV)
    routes_turns = jax.random.permutation(jax.random.fold_in(key_of[14], 3), SEQS // SEQ_DEV)
    routes = jax.vmap(lambda own, number: routed_block(jax.random.fold_in(key_of[14], 2), own, number, SEQ_DEV, EXPERTS, TOPK, CAP, 2))(routes_keys, routes_turns).reshape((SEQS, TOPK))
    route_weight = jnp.clip(jnp.exp(math.log(1.0) - 2.3025851 * jax.random.uniform(key_of[15], (SEQS, TOPK), jnp.float32) ** levels(key_of[15], (SEQS, TOPK), ((0, 64),), -0.2, 0.2)), 0.1, 1.0)
    expert_gate = noise(key_of[16], (EXPERTS, D, D_EXPERT), D ** -0.5, 0.125, ((0, 64), (2, 4)))
    expert_up = noise(key_of[17], (EXPERTS, D, D_EXPERT), D ** -0.5, 0.125, ((0, 64), (2, 4)))
    expert_down = noise(key_of[18], (EXPERTS, D_EXPERT, D), D_EXPERT ** -0.5, 0.25, ((0, 64), (1, 4)))
    shared_gate = noise(key_of[19], (D, D_SHARED), D ** -0.5, 0.125, ((0, 64), (1, 4)))
    shared_up = noise(key_of[20], (D, D_SHARED), D ** -0.5, 0.125, ((0, 64), (1, 4)))
    shared_down = noise(key_of[21], (D_SHARED, D), D_SHARED ** -0.5, 0.25, ((0, 4), (1, 64)))
    branch_gate = noise(key_of[22], (D,), D ** -0.5, 0.125)
    return dict(tokens=tokens, norm_gain=norm_gain, query_weight=query_weight, key_weight=key_weight, value_weight=value_weight, outgate_weight=outgate_weight, beta_weight=beta_weight, decay_weight=decay_weight, decay_rate=decay_rate, decay_bias=decay_bias, head_gain=head_gain, recurrent=recurrent, output_weight=output_weight, ffn_gain=ffn_gain, routes=routes, route_weight=route_weight, expert_gate=expert_gate, expert_up=expert_up, expert_down=expert_down, shared_gate=shared_gate, shared_up=shared_up, shared_down=shared_down, branch_gate=branch_gate)


EPS = 1e-06
ROUTED_SCALE = 2.5

def rms_scale(values, gain):
    values = values.astype(jnp.float32)
    return values * lax.rsqrt(lax.optimization_barrier(jnp.mean(values * values, axis=-1, keepdims=True)) + EPS) * gain.astype(jnp.float32)

def unit_rows(values):
    return values * lax.rsqrt(lax.optimization_barrier(jnp.sum(values * values, axis=-1, keepdims=True)) + EPS)

def grouped_product(left, right, groups):
    inner = left.shape[1] // groups
    running = jnp.zeros((left.shape[0], right.shape[1]), jnp.float32)
    for index in range(groups):
        partial_product = jnp.dot(left[:, index * inner:(index + 1) * inner], right[index * inner:(index + 1) * inner], preferred_element_type=jnp.float32)
        running = running + partial_product.astype(jnp.bfloat16).astype(jnp.float32)
    return running

def reference(tokens, norm_gain, query_weight, key_weight, value_weight, outgate_weight, beta_weight, decay_weight, decay_rate, decay_bias, head_gain, recurrent, output_weight, ffn_gain, routes, route_weight, expert_gate, expert_up, expert_down, shared_gate, shared_up, shared_down, branch_gate):
    seqs, width = tokens.shape
    heads, key_dim, value_dim = (recurrent.shape[1], recurrent.shape[2], recurrent.shape[3])
    key_heads = query_weight.shape[1] // key_dim
    normed = rms_scale(tokens, norm_gain).astype(jnp.bfloat16)
    query_proj = jnp.dot(normed, query_weight, preferred_element_type=jnp.float32).astype(jnp.bfloat16)
    key_proj = jnp.dot(normed, key_weight, preferred_element_type=jnp.float32).astype(jnp.bfloat16)
    value_proj = jnp.dot(normed, value_weight, preferred_element_type=jnp.float32).astype(jnp.bfloat16)
    gate_proj = jnp.dot(normed, outgate_weight, preferred_element_type=jnp.float32).astype(jnp.bfloat16)
    beta_logit = jnp.dot(normed, beta_weight, preferred_element_type=jnp.float32)
    decay_logit = jnp.dot(normed, decay_weight, preferred_element_type=jnp.float32)
    repeat_count = heads // key_heads
    queries = unit_rows(jax.nn.silu(query_proj.astype(jnp.float32)).reshape(seqs, key_heads, key_dim))
    queries = jnp.repeat(queries, repeat_count, axis=1) * key_dim ** (-0.5)
    key_rows = unit_rows(jax.nn.silu(key_proj.astype(jnp.float32)).reshape(seqs, key_heads, key_dim))
    key_rows = jnp.repeat(key_rows, repeat_count, axis=1)
    value_rows = jax.nn.silu(value_proj.astype(jnp.float32)).reshape(seqs, heads, value_dim)
    strength = jax.nn.sigmoid(beta_logit)
    retain = jnp.exp(-decay_rate[None, :] * jax.nn.softplus(decay_logit + decay_bias[None, :]))
    decayed = recurrent * retain[:, :, None, None]
    predicted = jnp.einsum('shde,shd->she', decayed, key_rows, precision=lax.Precision.HIGHEST)
    correction = strength[:, :, None] * (value_rows - predicted)
    new_state = decayed + key_rows[:, :, :, None] * correction[:, :, None, :]
    readout = jnp.einsum('shde,shd->she', new_state, queries, precision=lax.Precision.HIGHEST)
    out_gate = jax.nn.silu(gate_proj.astype(jnp.float32)).reshape(seqs, heads, value_dim)
    heads_out = (rms_scale(readout, head_gain) * out_gate).astype(jnp.bfloat16).reshape(seqs, heads * value_dim)
    mix = grouped_product(heads_out, output_weight, N_TP)
    residual = (tokens.astype(jnp.float32) + mix).astype(jnp.bfloat16)
    ffn_in = rms_scale(residual, ffn_gain).astype(jnp.bfloat16)
    topk = routes.shape[1]
    seq_local = seqs // N_EP
    experts_total = expert_gate.shape[0]
    pair_count = seq_local * topk
    pair_ids = routes.reshape(N_EP, pair_count).astype(jnp.int32)
    onehot = (pair_ids[:, :, None] == jnp.arange(experts_total).astype(jnp.int32)[None, None, :]).astype(jnp.int32)
    slots = lax.optimization_barrier(jnp.sum((jnp.cumsum(onehot, axis=1) - onehot) * onehot, axis=2)).astype(jnp.int32)
    target = (pair_ids * CAP + slots).astype(jnp.int32)
    source_rows = jnp.repeat(ffn_in.reshape(N_EP, seq_local, width), topk, axis=1)
    buffer = jnp.zeros((N_EP, experts_total * CAP, width), jnp.bfloat16)
    source_index = jnp.arange(N_EP).astype(jnp.int32)[:, None]
    buffer = buffer.at[source_index, target].set(source_rows)
    buffer = buffer.reshape(N_EP, experts_total, CAP, width).transpose(1, 0, 2, 3).reshape(experts_total, N_EP * CAP, width)

    def expert_rows(operands):
        rows_in, gate_matrix, up_matrix, down_matrix = operands
        gate_part = jnp.dot(rows_in, gate_matrix, preferred_element_type=jnp.float32)
        up_part = jnp.dot(rows_in, up_matrix, preferred_element_type=jnp.float32)
        act = (jax.nn.silu(gate_part) * up_part).astype(jnp.bfloat16)
        return grouped_product(act, down_matrix, N_TP).astype(jnp.bfloat16)
    results = lax.map(expert_rows, (buffer, expert_gate, expert_up, expert_down))
    results = results.reshape(experts_total, N_EP, CAP, width).transpose(1, 0, 2, 3).reshape(N_EP, experts_total * CAP, width)
    pair_out = jnp.take_along_axis(results, target[:, :, None], axis=1).astype(jnp.float32)
    scaled = route_weight / lax.optimization_barrier(jnp.sum(route_weight, axis=1, keepdims=True)) * ROUTED_SCALE
    moe = lax.optimization_barrier(jnp.sum(pair_out.reshape(seqs, topk, width) * scaled[:, :, None], axis=1))
    shared_g = jnp.dot(ffn_in, shared_gate, preferred_element_type=jnp.float32)
    shared_u = jnp.dot(ffn_in, shared_up, preferred_element_type=jnp.float32)
    shared_act = (jax.nn.silu(shared_g) * shared_u).astype(jnp.bfloat16)
    shared_out = grouped_product(shared_act, shared_down, N_TP)
    branch = jax.nn.sigmoid(jnp.dot(ffn_in, branch_gate, preferred_element_type=jnp.float32))
    layer_out = (residual.astype(jnp.float32) + moe + branch[:, None] * shared_out).astype(jnp.bfloat16)
    return (layer_out, new_state)
```

```python
import jax
import jax.numpy as jnp
from jax import lax
from jax.sharding import Mesh
from jax.sharding import PartitionSpec as P

EPS = 1e-06
ROUTED_SCALE = 2.5
BF = jnp.bfloat16
F32 = jnp.float32


def rms_scale(values, gain):
    values = values.astype(F32)
    return (
        values
        * lax.rsqrt(jnp.mean(values * values, axis=-1, keepdims=True) + EPS)
        * gain.astype(F32)
    )


def unit_rows(values):
    return values * lax.rsqrt(jnp.sum(values * values, axis=-1, keepdims=True) + EPS)


def exchange(pieces, axis):
    return lax.all_to_all(pieces, axis, split_axis=0, concat_axis=0, tiled=True)


def copies(array, axis):
    return jnp.broadcast_to(array, (lax.axis_size(axis), *array.shape))


def dot(a, b):
    return jnp.dot(a, b, preferred_element_type=F32)


def rows_from_all(piece):
    over_z = exchange(copies(piece, "z"), "z")
    over_y = exchange(copies(over_z, "y"), "y")
    other = lax.ppermute(over_y, "c", [(0, 1), (1, 0)])
    first = lax.axis_index("c") == 0
    both = jnp.stack([jnp.where(first, over_y, other), jnp.where(first, other, over_y)])
    return both.transpose(2, 1, 0, 3, 4).reshape(-1, piece.shape[1])


def per_device(
    tokens,
    norm_gain,
    query_weight,
    key_weight,
    value_weight,
    outgate_weight,
    beta_weight,
    decay_weight,
    decay_rate,
    decay_bias,
    head_gain,
    recurrent,
    output_weight,
    ffn_gain,
    routes,
    route_weight,
    expert_gate,
    expert_up,
    expert_down,
    shared_gate,
    shared_up,
    shared_down,
    branch_gate,
):
    nz, ny, nc = lax.axis_size("z"), lax.axis_size("y"), lax.axis_size("c")
    ep_count = nz * ny * nc
    seq_local, width = tokens.shape
    heads_local, key_dim, value_dim = recurrent.shape[1:]
    rows_k = query_weight.shape[0]
    block_k = ny * nc * rows_k

    weights = jnp.concatenate((query_weight, key_weight, value_weight, outgate_weight), axis=1)
    over_y = exchange(copies(weights, "y"), "y")
    normed = rms_scale(tokens, norm_gain).astype(BF)
    at = jnp.arange(block_k)
    src = (at // rows_k % ny) * (nc * rows_k) + (at // (rows_k * ny)) * rows_k + at % rows_k
    perm = (jnp.arange(block_k)[:, None] == src[None, :]).astype(BF)
    blocks = normed.reshape(seq_local, nz, block_k).transpose(1, 0, 2).reshape(nz * seq_local, block_k)
    blocks = dot(blocks, perm).astype(BF).reshape(nz, seq_local, block_k)
    arrived = exchange(blocks, "z").reshape(nz * seq_local, block_k)
    block_weights = lax.all_gather(over_y, "c", axis=0).reshape(block_k, weights.shape[1])
    partial = dot(arrived, block_weights).astype(BF).reshape(nz, seq_local, -1)
    proj = exchange(partial, "z").astype(F32).sum(axis=0).astype(BF).astype(F32)

    out_rows = rows_from_all(output_weight.T)
    shared_piece = jnp.concatenate((shared_gate, shared_up, shared_down.T), axis=1)
    shared_rows = rows_from_all(shared_piece)

    head_start = lax.axis_index("x") * heads_local
    beta_logit = dot(normed, lax.dynamic_slice_in_dim(beta_weight, head_start, heads_local, 1))
    decay_logit = dot(normed, lax.dynamic_slice_in_dim(decay_weight, head_start, heads_local, 1))
    strength = jax.nn.sigmoid(beta_logit)
    retain = jnp.exp(-decay_rate[None, :] * jax.nn.softplus(decay_logit + decay_bias[None, :]))

    nq, nv = query_weight.shape[1], value_weight.shape[1]
    key_local = nq // key_dim
    repeat_count = heads_local // key_local
    silu = jax.nn.silu(proj)
    queries = unit_rows(silu[:, :nq].reshape(seq_local, key_local, key_dim))
    queries = jnp.repeat(queries, repeat_count, axis=1) * key_dim ** (-0.5)
    key_rows = unit_rows(silu[:, nq : 2 * nq].reshape(seq_local, key_local, key_dim))
    key_rows = jnp.repeat(key_rows, repeat_count, axis=1)
    value_rows = silu[:, 2 * nq : 2 * nq + nv].reshape(seq_local, heads_local, value_dim)
    out_gate = silu[:, 2 * nq + nv :].reshape(seq_local, heads_local, value_dim)

    decayed = recurrent * retain[:, :, None, None]
    predicted = jnp.einsum("shde,shd->she", decayed, key_rows)
    correction = strength[:, :, None] * (value_rows - predicted)
    new_state = decayed + key_rows[:, :, :, None] * correction[:, :, None, :]
    readout = jnp.einsum("shde,shd->she", new_state, queries)
    heads_out = (
        (rms_scale(readout, head_gain) * out_gate)
        .astype(BF)
        .reshape(seq_local, heads_local * value_dim)
    )
    partial_mix = lax.dot_general(
        heads_out, out_rows, (((1,), (1,)), ((), ())), preferred_element_type=F32
    ).astype(BF)
    mixed = exchange(copies(partial_mix, "x"), "x").astype(F32).sum(axis=0)
    residual = (tokens.astype(F32) + mixed).astype(BF)
    ffn_in = rms_scale(residual, ffn_gain).astype(BF)

    topk = routes.shape[1]
    pair_count = seq_local * topk
    capacity = 2 * ((pair_count + ep_count - 1) // ep_count)
    expert_ids = routes.reshape(pair_count)
    onehot = (expert_ids[:, None] == jnp.arange(ep_count)[None, :]).astype(F32)
    earlier = (jnp.arange(pair_count)[:, None] > jnp.arange(pair_count)[None, :]).astype(F32)
    slots = jnp.sum(jnp.dot(earlier, onehot) * onehot, axis=1).astype(jnp.int32)
    target = (expert_ids * capacity + slots).reshape(seq_local, topk)
    place = target[:, :, None] == jnp.arange(ep_count * capacity)[None, None, :]
    scaled = route_weight / jnp.sum(route_weight, axis=1, keepdims=True) * ROUTED_SCALE
    dispatch = jnp.any(place, axis=1).astype(BF)
    combine = jnp.sum(jnp.where(place, scaled[:, :, None], 0.0), axis=1)
    combine_high = combine.astype(BF)
    combine_low = (combine - combine_high.astype(F32)).astype(BF)

    outgoing = dot(dispatch.T, ffn_in).astype(BF).reshape(ep_count, capacity, width)
    received = exchange(outgoing, ("z", "y", "c")).reshape(-1, width)
    act = (jax.nn.silu(dot(received, expert_gate[0])) * dot(received, expert_up[0])).astype(BF)
    partial_rows = dot(act, expert_down[0]).astype(BF).reshape(ep_count, capacity, width)
    returned = exchange(partial_rows, ("z", "y", "c")).reshape(-1, width)

    hidden = shared_gate.shape[1]
    shared_g = dot(ffn_in, shared_rows[:, :hidden])
    shared_u = dot(ffn_in, shared_rows[:, hidden : 2 * hidden])
    shared_act = (jax.nn.silu(shared_g) * shared_u).astype(BF)
    shared_part = lax.dot_general(
        shared_act, shared_rows[:, 2 * hidden :], (((1,), (1,)), ((), ())), preferred_element_type=F32
    )
    branch = jax.nn.sigmoid(dot(ffn_in, branch_gate))

    moe = dot(jnp.concatenate((combine_high, combine_low), axis=0), returned)
    moe = moe[:seq_local] + moe[seq_local:]
    addend = (moe + branch[:, None] * shared_part).astype(BF)
    summed = exchange(copies(addend, "x"), "x").astype(F32).sum(axis=0)
    layer_out = (residual.astype(F32) + summed).astype(BF)
    return (layer_out, new_state)


def solution(mesh):
    ep, tp = mesh.devices.shape
    fine = Mesh(mesh.devices.reshape(ep // 8, 4, 2, tp), ("z", "y", "c", "x"))
    E = ("z", "y", "c")
    return jax.shard_map(
        per_device,
        mesh=fine,
        in_specs=(
            P(E, None),
            P(),
            P(E, "x"),
            P(E, "x"),
            P(E, "x"),
            P(E, "x"),
            P(),
            P(),
            P("x"),
            P("x"),
            P(),
            P(E, "x", None, None),
            P("x", E),
            P(),
            P(E, None),
            P(E, None),
            P(E, None, "x"),
            P(E, None, "x"),
            P(E, "x", None),
            P(E, "x"),
            P(E, "x"),
            P("x", E),
            P(),
        ),
        out_specs=(P(E, None), P(E, "x", None, None)),
        check_vma=False,
    )
```

```python
import functools

import jax
import jax.numpy as jnp
from jax import lax
from jax.experimental import pallas as pl
from jax.experimental.pallas import tpu as pltpu
from jax.sharding import Mesh
from jax.sharding import PartitionSpec as P

EPS = 1e-06
ROUTED_SCALE = 2.5
BF = jnp.bfloat16
F32 = jnp.float32
VMEM = pl.BlockSpec(memory_space=pltpu.VMEM)
ANY = pl.BlockSpec(memory_space=pl.ANY)
NT = (((1,), (1,)), ((), ()))


def rms_scale(values, gain):
    values = values.astype(F32)
    return (
        values
        * lax.rsqrt(jnp.mean(values * values, axis=-1, keepdims=True) + EPS)
        * gain.astype(F32)
    )


def unit_rows(values):
    return values * lax.rsqrt(jnp.sum(values * values, axis=-1, keepdims=True) + EPS)


def exchange(pieces, axis):
    return lax.all_to_all(pieces, axis, split_axis=0, concat_axis=0, tiled=True)


def copies(array, axis):
    return jnp.broadcast_to(array, (lax.axis_size(axis), *array.shape))


def dot(a, b):
    return jnp.dot(a, b, preferred_element_type=F32)


def shifted(array, axis, by):
    n = lax.axis_size(axis)
    return lax.ppermute(array, axis, [(i, (i + by) % n) for i in range(n)])


def around_y_and_c(block):
    half = block.shape[0] // 2
    below = shifted(block, "y", 1)
    above = shifted(block, "y", -1)
    low, high = below[:half], above[half:]
    far_low = shifted(low, "y", 1)
    far_high = shifted(high, "y", -1)
    far = jnp.concatenate((far_low, far_high), axis=0)
    own = jnp.stack((block, below, far, above))
    return own, shifted(own, "c", 1)


def block_of(own_ref, other_ref, z, y, c):
    me_y, me_c = lax.axis_index("y"), lax.axis_index("c")
    at = lax.rem(me_y - y + 4, 4)
    return jnp.where(me_c == c, own_ref[at, z], other_ref[at, z])


def group_rows(own_ref, other_ref, group):
    z, first_y = group // 2, 2 * (group % 2)
    return jnp.concatenate(
        [block_of(own_ref, other_ref, z, first_y + i // 2, i % 2) for i in range(4)], axis=0
    )


def prep_kernel(tok_ref, gain_ref, wo_ref, out_ref, normed_ref):
    half = tok_ref.shape[0] // 2
    normed = rms_scale(tok_ref[...], gain_ref[...]).astype(BF)
    normed_ref[...] = normed
    peers, _, wide = out_ref.shape
    cols = wide // 2
    for z in range(peers):
        out_ref[z, 0:half, 0:cols] = normed[:half, z * cols : (z + 1) * cols]
        out_ref[z, 0:half, cols:wide] = normed[half:, z * cols : (z + 1) * cols]
        out_ref[z, half : half + wo_ref.shape[0], :] = wo_ref[...]


def delta_kernel(
    key_local, arr_ref, strength_ref, retain_ref, gain_ref, state_ref, new_hbm, heads_ref,
    new_ref, read_ref, sems,
):
    seqs, heads, key_dim, value_dim = state_ref.shape
    nq, nv = key_local * key_dim, heads * value_dim
    proj = jnp.sum(arr_ref[...].astype(F32), axis=0).astype(BF).astype(F32)
    silu = proj / (1.0 + jnp.exp(-proj))
    queries, keys = [], []
    for i in range(key_local):
        q = unit_rows(silu[:, i * key_dim : (i + 1) * key_dim]) * key_dim**-0.5
        k = unit_rows(silu[:, nq + i * key_dim : nq + (i + 1) * key_dim])
        queries.append(q.T)
        keys.append(k.T)
    strength, retain = strength_ref[...], retain_ref[...]
    outs = []
    for s in range(seqs):
        for h in range(heads):
            i = h * key_local // heads
            kc = keys[i][:, s : s + 1]
            qc = queries[i][:, s : s + 1]
            decayed = state_ref[s, h] * retain[s : s + 1, h : h + 1]
            predicted = jnp.sum(decayed * kc, axis=0, keepdims=True)
            at = 2 * nq + h * value_dim
            value = silu[s : s + 1, at : at + value_dim]
            correction = strength[s : s + 1, h : h + 1] * (value - predicted)
            new = decayed + kc * correction
            new_ref[s, h] = new
            read_ref[s : s + 1, h * value_dim : (h + 1) * value_dim] = jnp.sum(
                new * qc, axis=0, keepdims=True
            )
        out = pltpu.make_async_copy(new_ref.at[s], new_hbm.at[s], sems.at[s])
        out.start()
        outs.append(out)
    for h in range(heads):
        cols = slice(h * value_dim, (h + 1) * value_dim)
        gate = silu[:, 2 * nq + nv + h * value_dim : 2 * nq + nv + (h + 1) * value_dim]
        heads_ref[:, cols] = (rms_scale(read_ref[:, cols], gain_ref[...]) * gate).astype(BF)
    for out in outs:
        out.wait()


def mix_kernel(heads_ref, own_ref, other_ref, out_ref):
    heads = heads_ref[...]
    for group in range(out_ref.shape[2] // 128):
        rows = group_rows(own_ref, other_ref, group)
        part = lax.dot_general(heads, rows, NT, preferred_element_type=F32).astype(BF)
        for t in range(out_ref.shape[0]):
            out_ref[t, :, group * 128 : (group + 1) * 128] = part


def shared_kernel(hidden, rows_ref, branch_ref, own_ref, other_ref, out_ref):
    groups = out_ref.shape[1] // 128
    rows = rows_ref[...]
    total = jnp.zeros((rows.shape[0], 2 * hidden), F32)
    for group in range(groups):
        block = group_rows(own_ref.at[:, :, :, 0 : 2 * hidden], other_ref.at[:, :, :, 0 : 2 * hidden], group)
        total += dot(rows[:, group * 128 : (group + 1) * 128], block)
    gate, up = total[:, :hidden], total[:, hidden:]
    act = (gate / (1.0 + jnp.exp(-gate)) * up).astype(BF)
    logit = jnp.sum(rows.astype(F32) * branch_ref[...].astype(F32), axis=1, keepdims=True)
    branch = 1.0 / (1.0 + jnp.exp(-logit))
    for group in range(groups):
        block = group_rows(own_ref.at[:, :, :, 2 * hidden : 3 * hidden], other_ref.at[:, :, :, 2 * hidden : 3 * hidden], group)
        part = lax.dot_general(act, block, NT, preferred_element_type=F32)
        out_ref[:, group * 128 : (group + 1) * 128] = branch * part


def expert_kernel(rows_ref, gate_ref, up_ref, down_ref, out_ref):
    rows = rows_ref[...]
    gate = dot(rows, gate_ref[...])
    act = (gate / (1.0 + jnp.exp(-gate)) * dot(rows, up_ref[...])).astype(BF)
    out_ref[...] = dot(act, down_ref[...]).astype(BF)


def call(kernel, outs, args, flops, in_specs=None, out_specs=None, scratch=()):
    moved = sum(a.size * a.dtype.itemsize for a in args)
    shapes = [jax.ShapeDtypeStruct(shape, dtype) for shape, dtype in outs]
    return pl.pallas_call(
        kernel,
        out_shape=shapes,
        in_specs=in_specs or [VMEM] * len(args),
        out_specs=out_specs or [VMEM] * len(shapes),
        scratch_shapes=list(scratch),
        cost_estimate=pl.CostEstimate(flops=flops, bytes_accessed=moved, transcendentals=0),
        compiler_params=pltpu.CompilerParams(vmem_limit_bytes=24 * 1024 * 1024),
    )(*args)


def per_device(
    tokens,
    norm_gain,
    query_weight,
    key_weight,
    value_weight,
    outgate_weight,
    beta_weight,
    decay_weight,
    decay_rate,
    decay_bias,
    head_gain,
    recurrent,
    output_weight,
    ffn_gain,
    routes,
    route_weight,
    expert_gate,
    expert_up,
    expert_down,
    shared_gate,
    shared_up,
    shared_down,
    branch_gate,
):
    nz, ny, nc, nx = (lax.axis_size(a) for a in "zycx")
    ep_count = nz * ny * nc
    seqs, width = tokens.shape
    heads, key_dim, value_dim = recurrent.shape[1:]
    block_k = width // nz
    inner = heads * value_dim

    wo_rows = output_weight.T
    packed, normed = call(
        prep_kernel,
        [((nz, seqs // 2 + wo_rows.shape[0], 2 * block_k), BF), ((seqs, width), BF)],
        (tokens, norm_gain.reshape(1, width), wo_rows),
        1 << 20,
    )
    arrived = exchange(packed, "z")
    columns = arrived[:, : seqs // 2]
    columns = jnp.concatenate((columns[:, :, :block_k], columns[:, :, block_k:]), axis=1)
    wo_block = arrived[:, seqs // 2 :]

    weights = jnp.concatenate((query_weight, key_weight, value_weight, outgate_weight), axis=1)
    block_weights = lax.all_gather(weights, ("y", "c"), axis=0, tiled=True)
    partial = dot(columns.reshape(nz * seqs, block_k), block_weights).astype(BF)
    sums = exchange(partial.reshape(nz, seqs, -1), "z")

    wo_own, wo_other = around_y_and_c(wo_block)

    head_start = lax.axis_index("x") * heads
    beta_logit = dot(normed, lax.dynamic_slice_in_dim(beta_weight, head_start, heads, 1))
    decay_logit = dot(normed, lax.dynamic_slice_in_dim(decay_weight, head_start, heads, 1))
    strength = jax.nn.sigmoid(beta_logit)
    retain = jnp.exp(-decay_rate[None, :] * jax.nn.softplus(decay_logit + decay_bias[None, :]))

    new_state, heads_out = call(
        functools.partial(delta_kernel, query_weight.shape[1] // key_dim),
        [(recurrent.shape, F32), ((seqs, inner), BF)],
        (sums, strength, retain, head_gain.reshape(1, value_dim), recurrent),
        1 << 26,
        out_specs=[ANY, VMEM],
        scratch=[
            pltpu.VMEM(recurrent.shape, F32),
            pltpu.VMEM((seqs, inner), F32),
            pltpu.SemaphoreType.DMA((seqs,)),
        ],
    )
    (mix_copies,) = call(
        mix_kernel, [((nx, seqs, width), BF)], (heads_out, wo_own, wo_other), 1 << 25
    )
    mixed = exchange(mix_copies, "x").astype(F32).sum(axis=0)
    residual = (tokens.astype(F32) + mixed).astype(BF)
    ffn_in = rms_scale(residual, ffn_gain).astype(BF)

    topk = routes.shape[1]
    pair_count = seqs * topk
    capacity = 2 * ((pair_count + ep_count - 1) // ep_count)
    expert_ids = routes.reshape(pair_count)
    onehot = (expert_ids[:, None] == jnp.arange(ep_count)[None, :]).astype(F32)
    earlier = (jnp.arange(pair_count)[:, None] > jnp.arange(pair_count)[None, :]).astype(F32)
    slots = jnp.sum(jnp.dot(earlier, onehot) * onehot, axis=1).astype(jnp.int32)
    target = (expert_ids * capacity + slots).reshape(seqs, topk)
    place = target[:, :, None] == jnp.arange(ep_count * capacity)[None, None, :]
    scaled = route_weight / jnp.sum(route_weight, axis=1, keepdims=True) * ROUTED_SCALE
    dispatch = jnp.any(place, axis=1).astype(BF)
    combine = jnp.sum(jnp.where(place, scaled[:, :, None], 0.0), axis=1)
    combine_high = combine.astype(BF)
    combine_low = (combine - combine_high.astype(F32)).astype(BF)

    outgoing = dot(dispatch.T, ffn_in).astype(BF).reshape(ep_count, capacity, width)
    received = exchange(outgoing, ("z", "y", "c")).reshape(-1, width)

    shared_piece = jnp.concatenate((shared_gate, shared_up, shared_down.T), axis=1)
    shared_piece, ffn_tied = lax.optimization_barrier((shared_piece, ffn_in))
    shared_block = lax.all_gather(shared_piece, ("z", "c"), axis=0)
    shared_block = shared_block.reshape(nz, nc, *shared_piece.shape)
    shared_block = lax.dynamic_index_in_dim(shared_block, lax.axis_index("c"), 1, keepdims=False)

    (partial_rows,) = call(
        expert_kernel,
        [((ep_count * capacity, width), BF)],
        (received, expert_gate[0], expert_up[0], expert_down[0]),
        1 << 28,
    )
    returned = exchange(partial_rows.reshape(ep_count, capacity, width), ("z", "y", "c"))
    returned = returned.reshape(-1, width)

    shared_own, shared_other = around_y_and_c(shared_block)
    (shared_part,) = call(
        functools.partial(shared_kernel, shared_gate.shape[1]),
        [((seqs, width), F32)],
        (ffn_tied, branch_gate.reshape(1, width), shared_own, shared_other),
        1 << 25,
    )

    moe = dot(jnp.concatenate((combine_high, combine_low), axis=0), returned)
    addend = (moe[:seqs] + moe[seqs:] + shared_part).astype(BF)
    summed = exchange(copies(addend, "x"), "x").astype(F32).sum(axis=0)
    layer_out = (residual.astype(F32) + summed).astype(BF)
    return (layer_out, new_state)


def solution(mesh):
    ep, tp = mesh.devices.shape
    fine = Mesh(mesh.devices.reshape(ep // 8, 4, 2, tp), ("z", "y", "c", "x"))
    E = ("z", "y", "c")
    return jax.shard_map(
        per_device,
        mesh=fine,
        in_specs=(
            P(E, None),
            P(),
            P(E, "x"),
            P(E, "x"),
            P(E, "x"),
            P(E, "x"),
            P(),
            P(),
            P("x"),
            P("x"),
            P(),
            P(E, "x", None, None),
            P("x", E),
            P(),
            P(E, None),
            P(E, None),
            P(E, None, "x"),
            P(E, None, "x"),
            P(E, "x", None),
            P(E, "x"),
            P(E, "x"),
            P("x", E),
            P(),
        ),
        out_specs=(P(E, None), P(E, "x", None, None)),
        check_vma=False,
    )
```

```python
import functools

import jax
import jax.numpy as jnp
from jax import lax
from jax.experimental import pallas as pl
from jax.experimental.pallas import tpu as pltpu
from jax.sharding import Mesh
from jax.sharding import PartitionSpec as P

EPS = 1e-06
ROUTED_SCALE = 2.5
BF = jnp.bfloat16
F32 = jnp.float32
VMEM = pl.BlockSpec(memory_space=pltpu.VMEM)
HBM = pl.BlockSpec(memory_space=pltpu.HBM)
NT = (((1,), (1,)), ((), ()))


def rms_scale(values, gain):
    values = values.astype(F32)
    return (
        values
        * lax.rsqrt(jnp.mean(values * values, axis=-1, keepdims=True) + EPS)
        * gain.astype(F32)
    )


def unit_rows(values):
    return values * lax.rsqrt(jnp.sum(values * values, axis=-1, keepdims=True) + EPS)


def exchange(pieces, axis):
    return lax.all_to_all(pieces, axis, split_axis=0, concat_axis=0, tiled=True)


def copies(array, axis):
    return jnp.broadcast_to(array, (lax.axis_size(axis), *array.shape))


def dot(a, b):
    return jnp.dot(a, b, preferred_element_type=F32)


def shifted(array, axis, by):
    n = lax.axis_size(axis)
    return lax.ppermute(array, axis, [(i, (i + by) % n) for i in range(n)])


def around_y_and_c(block):
    half = block.shape[0] // 2
    below = shifted(block, "y", 1)
    above = shifted(block, "y", -1)
    low, high = below[:half], above[half:]
    far_low = shifted(low, "y", 1)
    far_high = shifted(high, "y", -1)
    far = jnp.concatenate((far_low, far_high), axis=0)
    own = jnp.stack((block, below, far, above))
    return own, shifted(own, "c", 1)


def block_of(own_ref, other_ref, z, y, c):
    me_y, me_c = lax.axis_index("y"), lax.axis_index("c")
    at = lax.rem(me_y - y + 4, 4)
    return jnp.where(me_c == c, own_ref[at, z], other_ref[at, z])


def group_rows(own_ref, other_ref, group):
    z, first_y = group // 2, 2 * (group % 2)
    return jnp.concatenate(
        [block_of(own_ref, other_ref, z, first_y + i // 2, i % 2) for i in range(4)], axis=0
    )


def fetched(sources, targets, sems):
    moves = [pltpu.make_async_copy(a, b, sems.at[i]) for i, (a, b) in enumerate(zip(sources, targets))]
    for move in moves:
        move.start()
    for move in moves:
        move.wait()


def pack_kernel(count, *refs):
    sources, out_ref, sems = refs[:count], refs[count], refs[count + 1]
    targets, at = [], 0
    for source in sources:
        targets.append(out_ref.at[:, at : at + source.shape[1]])
        at += source.shape[1]
    fetched(sources, targets, sems)


def prep_kernel(*refs):
    fetched(refs[:6], refs[8:14], refs[14])
    out_ref, normed_ref = refs[6:8]
    tok_ref, gain_ref, wo_ref, gate_ref, up_ref, down_ref = refs[8:14]
    half = tok_ref.shape[0] // 2
    normed = rms_scale(tok_ref[...], gain_ref[...]).astype(BF)
    normed_ref[...] = normed
    peers, _, wide = out_ref.shape
    cols = wide // 2
    rows, hidden = gate_ref.shape
    for z in range(peers):
        at = half
        out_ref[z, 0:half, 0:cols] = normed[:half, z * cols : (z + 1) * cols]
        out_ref[z, 0:half, cols:wide] = normed[half:, z * cols : (z + 1) * cols]
        out_ref[z, at : at + rows, :] = wo_ref[...]
        at += rows
        for i in range(2):
            part = slice(i * rows // 2, (i + 1) * rows // 2)
            out_ref[z, at : at + rows // 2, 2 * i * hidden : (2 * i + 1) * hidden] = gate_ref[part]
            out_ref[z, at : at + rows // 2, (2 * i + 1) * hidden : (2 * i + 2) * hidden] = up_ref[part]
        at += rows // 2
        for i in range(4):
            part = slice(i * rows // 4, (i + 1) * rows // 4)
            out_ref[z, at : at + rows // 4, i * hidden : (i + 1) * hidden] = down_ref[part]


def proj_kernel(arr_ref, own_ref, other_ref, out_ref):
    peers, seqs, _ = out_ref.shape
    half = seqs // 2
    cols = arr_ref.shape[2] // 2
    parts = []
    for z in range(peers):
        parts += [arr_ref[z, 0:half, 0:cols], arr_ref[z, 0:half, cols : 2 * cols]]
    rows = jnp.concatenate(parts, axis=0)
    me_y, me_c = lax.axis_index("y"), lax.axis_index("c")
    blocks = []
    for i in range(8):
        at = lax.rem(me_y - i // 2 + 4, 4)
        blocks.append(jnp.where(me_c == i % 2, own_ref[at], other_ref[at]))
    part = dot(rows, jnp.concatenate(blocks, axis=0)).astype(BF)
    for z in range(peers):
        out_ref[z] = part[z * seqs : (z + 1) * seqs]


def delta_kernel(
    key_local, arr_ref, strength_ref, retain_ref, gain_ref, state_hbm, new_hbm, heads_ref,
    state_ref, new_ref, read_ref, in_sems, sems,
):
    seqs, heads, key_dim, value_dim = state_ref.shape
    ins = [pltpu.make_async_copy(state_hbm.at[s], state_ref.at[s], in_sems.at[s]) for s in range(seqs)]
    for copy in ins:
        copy.start()
    nq, nv = key_local * key_dim, heads * value_dim
    proj = jnp.sum(arr_ref[...].astype(F32), axis=0).astype(BF).astype(F32)
    silu = proj / (1.0 + jnp.exp(-proj))
    queries, keys = [], []
    for i in range(key_local):
        q = unit_rows(silu[:, i * key_dim : (i + 1) * key_dim]) * key_dim**-0.5
        k = unit_rows(silu[:, nq + i * key_dim : nq + (i + 1) * key_dim])
        queries.append(q.T)
        keys.append(k.T)
    strength, retain = strength_ref[...], retain_ref[...]
    outs = []
    for s in range(seqs):
        ins[s].wait()
        for h in range(heads):
            i = h * key_local // heads
            kc = keys[i][:, s : s + 1]
            qc = queries[i][:, s : s + 1]
            decayed = state_ref[s, h] * retain[s : s + 1, h : h + 1]
            predicted = jnp.sum(decayed * kc, axis=0, keepdims=True)
            at = 2 * nq + h * value_dim
            value = silu[s : s + 1, at : at + value_dim]
            correction = strength[s : s + 1, h : h + 1] * (value - predicted)
            new = decayed + kc * correction
            new_ref[s, h] = new
            read_ref[s : s + 1, h * value_dim : (h + 1) * value_dim] = jnp.sum(
                new * qc, axis=0, keepdims=True
            )
        out = pltpu.make_async_copy(new_ref.at[s], new_hbm.at[s], sems.at[s])
        out.start()
        outs.append(out)
    for h in range(heads):
        cols = slice(h * value_dim, (h + 1) * value_dim)
        gate = silu[:, 2 * nq + nv + h * value_dim : 2 * nq + nv + (h + 1) * value_dim]
        heads_ref[:, cols] = (rms_scale(read_ref[:, cols], gain_ref[...]) * gate).astype(BF)
    for out in outs:
        out.wait()


def mix_kernel(heads_ref, own_ref, other_ref, out_ref):
    heads = heads_ref[...]
    for group in range(out_ref.shape[2] // 128):
        rows = group_rows(own_ref, other_ref, group)
        part = lax.dot_general(heads, rows, NT, preferred_element_type=F32).astype(BF)
        for t in range(out_ref.shape[0]):
            out_ref[t, :, group * 128 : (group + 1) * 128] = part


def shared_kernel(rows_ref, branch_ref, own_ref, other_ref, out_ref):
    groups = out_ref.shape[1] // 128
    hidden = own_ref.shape[3] // 4
    rows = rows_ref[...]
    total = jnp.zeros((rows.shape[0], 2 * hidden), F32)
    downs = []
    for group in range(groups):
        z, first_y = group // 2, 2 * (group % 2)
        block, down = [], []
        for i in range(4):
            piece = block_of(own_ref, other_ref, z, first_y + i // 2, i % 2)
            half = piece.shape[0] * 2 // 3
            block += [piece[:half, : 2 * hidden], piece[:half, 2 * hidden :]]
            down += [piece[half:, j * hidden : (j + 1) * hidden] for j in range(4)]
        downs.append(jnp.concatenate(down, axis=0))
        total += dot(rows[:, group * 128 : (group + 1) * 128], jnp.concatenate(block, axis=0))
    gate, up = total[:, :hidden], total[:, hidden:]
    act = (gate / (1.0 + jnp.exp(-gate)) * up).astype(BF)
    logit = jnp.sum(rows.astype(F32) * branch_ref[...].astype(F32), axis=1, keepdims=True)
    branch = 1.0 / (1.0 + jnp.exp(-logit))
    for group in range(groups):
        part = lax.dot_general(act, downs[group], NT, preferred_element_type=F32)
        out_ref[:, group * 128 : (group + 1) * 128] = branch * part


def expert_kernel(rows_ref, gate_ref, up_ref, down_ref, out_ref):
    rows = rows_ref[...]
    gate = dot(rows, gate_ref[...])
    act = (gate / (1.0 + jnp.exp(-gate)) * dot(rows, up_ref[...])).astype(BF)
    out_ref[...] = dot(act, down_ref[...]).astype(BF)


def call(kernel, outs, args, flops, in_specs=None, out_specs=None, scratch=(), limit=16):
    moved = sum(a.size * a.dtype.itemsize for a in args)
    shapes = [jax.ShapeDtypeStruct(shape, dtype) for shape, dtype in outs]
    return pl.pallas_call(
        kernel,
        out_shape=shapes,
        in_specs=in_specs or [VMEM] * len(args),
        out_specs=out_specs or [VMEM] * len(shapes),
        scratch_shapes=list(scratch),
        cost_estimate=pl.CostEstimate(flops=flops, bytes_accessed=moved, transcendentals=0),
        compiler_params=pltpu.CompilerParams(vmem_limit_bytes=limit << 20),
    )(*args)


def per_device(
    tokens,
    norm_gain,
    query_weight,
    key_weight,
    value_weight,
    outgate_weight,
    beta_weight,
    decay_weight,
    decay_rate,
    decay_bias,
    head_gain,
    recurrent,
    output_weight,
    ffn_gain,
    routes,
    route_weight,
    expert_gate,
    expert_up,
    expert_down,
    shared_gate,
    shared_up,
    shared_down,
    branch_gate,
):
    nz, ny, nc, nx = (lax.axis_size(a) for a in "zycx")
    ep_count = nz * ny * nc
    seqs, width = tokens.shape
    heads, key_dim, value_dim = recurrent.shape[1:]
    block_k = width // nz
    inner = heads * value_dim

    pieces = (query_weight, key_weight, value_weight, outgate_weight)
    (weights,) = call(
        functools.partial(pack_kernel, len(pieces)),
        [((query_weight.shape[0], sum(w.shape[1] for w in pieces)), BF)],
        pieces,
        1 << 20,
        in_specs=[HBM] * len(pieces),
        limit=60,
        scratch=[pltpu.SemaphoreType.DMA((len(pieces),))],
    )
    w_own, w_other = around_y_and_c(weights)

    wo_rows = output_weight.T
    half, rows = seqs // 2, wo_rows.shape[0]
    depth = half + rows + rows // 2 + rows // 4
    inputs = (tokens, norm_gain.reshape(1, width), wo_rows, shared_gate, shared_up, shared_down.T)
    packed, normed = call(
        prep_kernel,
        [((nz, depth, 2 * block_k), BF), ((seqs, width), BF)],
        inputs,
        1 << 20,
        in_specs=[HBM] * len(inputs),
        limit=60,
        scratch=[pltpu.VMEM(a.shape, BF) for a in inputs] + [pltpu.SemaphoreType.DMA((len(inputs),))],
    )
    arrived = exchange(packed, "z")
    wo_block = arrived[:, half : half + rows]
    shared_block = arrived[:, half + rows :]

    (partial,) = call(
        proj_kernel, [((nz, seqs, weights.shape[1]), BF)], (arrived, w_own, w_other), 1 << 26
    )
    sums = exchange(partial, "z")

    wo_own, wo_other = around_y_and_c(wo_block)

    head_start = lax.axis_index("x") * heads
    beta_logit = dot(normed, lax.dynamic_slice_in_dim(beta_weight, head_start, heads, 1))
    decay_logit = dot(normed, lax.dynamic_slice_in_dim(decay_weight, head_start, heads, 1))
    strength = jax.nn.sigmoid(beta_logit)
    retain = jnp.exp(-decay_rate[None, :] * jax.nn.softplus(decay_logit + decay_bias[None, :]))

    new_state, heads_out = call(
        functools.partial(delta_kernel, query_weight.shape[1] // key_dim),
        [(recurrent.shape, F32), ((seqs, inner), BF)],
        (sums, strength, retain, head_gain.reshape(1, value_dim), recurrent),
        1 << 26,
        in_specs=[VMEM, VMEM, VMEM, VMEM, HBM],
        out_specs=[HBM, VMEM],
        limit=52,
        scratch=[
            pltpu.VMEM(recurrent.shape, F32),
            pltpu.VMEM(recurrent.shape, F32),
            pltpu.VMEM((seqs, inner), F32),
            pltpu.SemaphoreType.DMA((seqs,)),
            pltpu.SemaphoreType.DMA((seqs,)),
        ],
    )
    (mix_copies,) = call(
        mix_kernel, [((nx, seqs, width), BF)], (heads_out, wo_own, wo_other), 1 << 25
    )
    mixed = exchange(mix_copies, "x").astype(F32).sum(axis=0)
    residual = (tokens.astype(F32) + mixed).astype(BF)
    ffn_in = rms_scale(residual, ffn_gain).astype(BF)

    topk = routes.shape[1]
    pair_count = seqs * topk
    capacity = 2 * ((pair_count + ep_count - 1) // ep_count)
    expert_ids = routes.reshape(pair_count)
    onehot = (expert_ids[:, None] == jnp.arange(ep_count)[None, :]).astype(F32)
    earlier = (jnp.arange(pair_count)[:, None] > jnp.arange(pair_count)[None, :]).astype(F32)
    slots = jnp.sum(jnp.dot(earlier, onehot) * onehot, axis=1).astype(jnp.int32)
    target = (expert_ids * capacity + slots).reshape(seqs, topk)
    place = target[:, :, None] == jnp.arange(ep_count * capacity)[None, None, :]
    scaled = route_weight / jnp.sum(route_weight, axis=1, keepdims=True) * ROUTED_SCALE
    dispatch = jnp.any(place, axis=1).astype(BF)
    combine = jnp.sum(jnp.where(place, scaled[:, :, None], 0.0), axis=1)
    combine_high = combine.astype(BF)
    combine_low = (combine - combine_high.astype(F32)).astype(BF)

    outgoing = dot(dispatch.T, ffn_in).astype(BF).reshape(ep_count, capacity, width)
    received = exchange(outgoing, ("z", "y", "c")).reshape(-1, width)

    (partial_rows,) = call(
        expert_kernel,
        [((ep_count * capacity, width), BF)],
        (received, expert_gate[0], expert_up[0], expert_down[0]),
        1 << 28,
    )
    returned = exchange(partial_rows.reshape(ep_count, capacity, width), ("z", "y", "c"))
    returned = returned.reshape(-1, width)

    shared_own, shared_other = around_y_and_c(shared_block)
    (shared_part,) = call(
        shared_kernel,
        [((seqs, width), F32)],
        (ffn_in, branch_gate.reshape(1, width), shared_own, shared_other),
        1 << 25,
    )

    moe = dot(jnp.concatenate((combine_high, combine_low), axis=0), returned)
    addend = (moe[:seqs] + moe[seqs:] + shared_part).astype(BF)
    summed = exchange(copies(addend, "x"), "x").astype(F32).sum(axis=0)
    layer_out = (residual.astype(F32) + summed).astype(BF)
    return (layer_out, new_state)


def solution(mesh):
    ep, tp = mesh.devices.shape
    fine = Mesh(mesh.devices.reshape(ep // 8, 4, 2, tp), ("z", "y", "c", "x"))
    E = ("z", "y", "c")
    return jax.shard_map(
        per_device,
        mesh=fine,
        in_specs=(
            P(E, None),
            P(),
            P(E, "x"),
            P(E, "x"),
            P(E, "x"),
            P(E, "x"),
            P(),
            P(),
            P("x"),
            P("x"),
            P(),
            P(E, "x", None, None),
            P("x", E),
            P(),
            P(E, None),
            P(E, None),
            P(E, None, "x"),
            P(E, None, "x"),
            P(E, "x", None),
            P(E, "x"),
            P(E, "x"),
            P("x", E),
            P(),
        ),
        out_specs=(P(E, None), P(E, "x", None, None)),
        check_vma=False,
    )
```

```python
import functools

import jax
import jax.numpy as jnp
from jax import lax
from jax.experimental import pallas as pl
from jax.experimental.pallas import tpu as pltpu
from jax.sharding import Mesh
from jax.sharding import PartitionSpec as P

EPS = 1e-06
ROUTED_SCALE = 2.5
BF = jnp.bfloat16
F32 = jnp.float32
VMEM = pl.BlockSpec(memory_space=pltpu.VMEM)
HBM = pl.BlockSpec(memory_space=pltpu.HBM)
NT = (((1,), (1,)), ((), ()))


def rms_scale(values, gain):
    values = values.astype(F32)
    return (
        values
        * lax.rsqrt(jnp.mean(values * values, axis=-1, keepdims=True) + EPS)
        * gain.astype(F32)
    )


def unit_rows(values):
    return values * lax.rsqrt(jnp.sum(values * values, axis=-1, keepdims=True) + EPS)


def exchange(pieces, axis):
    return lax.all_to_all(pieces, axis, split_axis=0, concat_axis=0, tiled=True)


def dot(a, b):
    return jnp.dot(a, b, preferred_element_type=F32)


def shifted(array, axis, by):
    n = lax.axis_size(axis)
    return lax.ppermute(array, axis, [(i, (i + by) % n) for i in range(n)])


def around_y(block, cut):
    below = shifted(block, "y", 1)
    above = shifted(block, "y", -1)
    far_low = shifted(below[:cut], "y", 1)
    far_high = shifted(above[cut:], "y", -1)
    return block, below, (far_low, far_high), above


def around_y_and_c(block):
    below = shifted(block, "y", 1)
    above = shifted(block, "y", -1)
    far = shifted(below, "y", 1)
    own = jnp.stack((block, below, far, above))
    return own, shifted(own, "c", 1)


def total_over_x(part):
    return [part] + [shifted(part, "x", i) for i in (2, 1, 3)]


def four(a_ref, b_ref, c_ref, d_ref):
    a, b, c, d = (r[...].astype(F32) for r in (a_ref, b_ref, c_ref, d_ref))
    return (a + b) + (c + d)


def block_of(refs, z, y, c):
    near_ref, other_near_ref, *fars = refs
    at = lax.rem(lax.axis_index("y") - y + 4, 4)
    near = jnp.minimum(at, 2)
    mine = lax.axis_index("c") == c
    here = jnp.where(mine, near_ref[near, z], other_near_ref[near, z])
    half = fars[0].shape[0]
    far = jnp.where(mine, fars[z // half][z % half], fars[2 + z // half][z % half])
    return jnp.where(at == 2, far, here)


def group_rows(refs, group):
    z, first_y = group // 2, 2 * (group % 2)
    return jnp.concatenate(
        [block_of(refs, z, first_y + i // 2, i % 2) for i in range(4)], axis=0
    )


def prep_kernel(*refs):
    sources, (out_ref, normed_ref, weights_ref), targets = refs[:10], refs[10:13], list(refs[13:19])
    tok_ref, gain_ref, wo_ref, gate_ref, up_ref, down_ref = targets
    at = 0
    for source in sources[6:]:
        targets.append(weights_ref.at[:, at : at + source.shape[1]])
        at += source.shape[1]
    moves = [
        pltpu.make_async_copy(source, target, refs[19].at[i])
        for i, (source, target) in enumerate(zip(sources, targets))
    ]
    for move in moves:
        move.start()
    for move in moves[:6]:
        move.wait()
    half = tok_ref.shape[0] // 2
    values = tok_ref[...].astype(F32)
    scale = lax.rsqrt(jnp.mean(values * values, axis=-1, keepdims=True) + EPS)
    gain = gain_ref[...].astype(F32)
    peers, _, wide = out_ref.shape
    cols = wide // 2
    rows, hidden = gate_ref.shape
    for j in range(gain.shape[0]):
        lanes = slice(j * 128, (j + 1) * 128)
        part = (values[:, lanes] * scale * gain[j : j + 1]).astype(BF)
        normed_ref[:, lanes] = part
        z, at = j * 128 // cols, j * 128 % cols
        out_ref[z, 0:half, at : at + 128] = part[:half]
        out_ref[z, 0:half, cols + at : cols + at + 128] = part[half:]
    for z in range(peers):
        at = half
        out_ref[z, at : at + rows, :] = wo_ref[...]
        at += rows
        for i in range(2):
            part = slice(i * rows // 2, (i + 1) * rows // 2)
            out_ref[z, at : at + rows // 2, 2 * i * hidden : (2 * i + 1) * hidden] = gate_ref[part]
            out_ref[z, at : at + rows // 2, (2 * i + 1) * hidden : (2 * i + 2) * hidden] = up_ref[part]
        at += rows // 2
        for i in range(4):
            part = slice(i * rows // 4, (i + 1) * rows // 4)
            out_ref[z, at : at + rows // 4, i * hidden : (i + 1) * hidden] = down_ref[part]
    for move in moves[6:]:
        move.wait()


def proj_kernel(arr_ref, own_ref, other_ref, out_ref):
    peers, seqs, _ = out_ref.shape
    half = seqs // 2
    cols = arr_ref.shape[2] // 2
    parts = []
    for z in range(peers):
        parts += [arr_ref[z, 0:half, 0:cols], arr_ref[z, 0:half, cols : 2 * cols]]
    rows = jnp.concatenate(parts, axis=0)
    me_y, me_c = lax.axis_index("y"), lax.axis_index("c")
    blocks = []
    for i in range(8):
        at = lax.rem(me_y - i // 2 + 4, 4)
        blocks.append(jnp.where(me_c == i % 2, own_ref[at], other_ref[at]))
    part = dot(rows, jnp.concatenate(blocks, axis=0)).astype(BF)
    for z in range(peers):
        out_ref[z] = part[z * seqs : (z + 1) * seqs]


def delta_kernel(
    key_local, arr_ref, strength_ref, retain_ref, gain_ref, state_hbm, new_hbm, heads_ref,
    state_ref, new_ref, read_ref, in_sems, sems,
):
    seqs, heads, key_dim, value_dim = state_ref.shape
    ins = [pltpu.make_async_copy(state_hbm.at[s], state_ref.at[s], in_sems.at[s]) for s in range(seqs)]
    ahead = 10
    for copy in ins[:ahead]:
        copy.start()
    nq, nv = key_local * key_dim, heads * value_dim
    proj = jnp.sum(arr_ref[...].astype(F32), axis=0).astype(BF).astype(F32)
    silu = proj / (1.0 + jnp.exp(-proj))
    queries, keys = [], []
    for i in range(key_local):
        q = unit_rows(silu[:, i * key_dim : (i + 1) * key_dim]) * key_dim**-0.5
        k = unit_rows(silu[:, nq + i * key_dim : nq + (i + 1) * key_dim])
        queries.append(q.T)
        keys.append(k.T)
    strength, retain = strength_ref[...], retain_ref[...]
    outs = []
    for s in range(seqs):
        ins[s].wait()
        if s + ahead < seqs:
            ins[s + ahead].start()
        for h in range(heads):
            i = h * key_local // heads
            kc = keys[i][:, s : s + 1]
            qc = queries[i][:, s : s + 1]
            decayed = state_ref[s, h] * retain[s : s + 1, h : h + 1]
            predicted = jnp.sum(decayed * kc, axis=0, keepdims=True)
            at = 2 * nq + h * value_dim
            value = silu[s : s + 1, at : at + value_dim]
            correction = strength[s : s + 1, h : h + 1] * (value - predicted)
            new = decayed + kc * correction
            new_ref[s, h] = new
            read_ref[s : s + 1, h * value_dim : (h + 1) * value_dim] = jnp.sum(
                new * qc, axis=0, keepdims=True
            )
        out = pltpu.make_async_copy(new_ref.at[s], new_hbm.at[s], sems.at[s])
        out.start()
        outs.append(out)
    for h in range(heads):
        cols = slice(h * value_dim, (h + 1) * value_dim)
        gate = silu[:, 2 * nq + nv + h * value_dim : 2 * nq + nv + (h + 1) * value_dim]
        heads_ref[:, cols] = (rms_scale(read_ref[:, cols], gain_ref[...]) * gate).astype(BF)
    for out in outs:
        out.wait()


def mix_kernel(heads_ref, *refs):
    heads, out_ref = heads_ref[...], refs[6]
    for group in range(out_ref.shape[1] // 128):
        rows = group_rows(refs[:6], group)
        part = lax.dot_general(heads, rows, NT, preferred_element_type=F32)
        out_ref[:, group * 128 : (group + 1) * 128] = part.astype(BF)


def post_kernel(a_ref, b_ref, c_ref, d_ref, tok_ref, gain_ref, dispatch_ref, res_ref, ffn_ref, out_ref):
    residual = (tok_ref[...].astype(F32) + four(a_ref, b_ref, c_ref, d_ref)).astype(BF)
    res_ref[...] = residual
    ffn_in = rms_scale(residual, gain_ref[...]).astype(BF)
    ffn_ref[...] = ffn_in
    out_ref[...] = lax.dot_general(
        dispatch_ref[...], ffn_in, (((0,), (0,)), ((), ())), preferred_element_type=F32
    ).astype(BF).reshape(out_ref.shape)


def final_kernel(a_ref, b_ref, c_ref, d_ref, res_ref, out_ref):
    out_ref[...] = (res_ref[...].astype(F32) + four(a_ref, b_ref, c_ref, d_ref)).astype(BF)


def shared_kernel(rows_ref, branch_ref, own_ref, other_ref, out_ref):
    groups = out_ref.shape[1] // 128
    hidden = own_ref.shape[3] // 4
    rows = rows_ref[...]
    total = jnp.zeros((rows.shape[0], 2 * hidden), F32)
    downs = []
    for group in range(groups):
        z, first_y = group // 2, 2 * (group % 2)
        block, down = [], []
        for i in range(4):
            at_y = lax.rem(lax.axis_index("y") - first_y - i // 2 + 4, 4)
            mine = lax.axis_index("c") == i % 2
            piece = jnp.where(mine, own_ref[at_y, z], other_ref[at_y, z])
            half = piece.shape[0] * 2 // 3
            block += [piece[:half, : 2 * hidden], piece[:half, 2 * hidden :]]
            down += [piece[half:, j * hidden : (j + 1) * hidden] for j in range(4)]
        downs.append(jnp.concatenate(down, axis=0))
        total += dot(rows[:, group * 128 : (group + 1) * 128], jnp.concatenate(block, axis=0))
    gate, up = total[:, :hidden], total[:, hidden:]
    act = (gate / (1.0 + jnp.exp(-gate)) * up).astype(BF)
    logit = jnp.sum(rows.astype(F32) * branch_ref[...].astype(F32), axis=1, keepdims=True)
    branch = 1.0 / (1.0 + jnp.exp(-logit))
    for group in range(groups):
        part = lax.dot_general(act, downs[group], NT, preferred_element_type=F32)
        out_ref[:, group * 128 : (group + 1) * 128] = branch * part


def expert_kernel(rows_ref, gate_up_ref, down_ref, out_ref):
    both = dot(rows_ref[...], gate_up_ref[...])
    hidden = both.shape[1] // 2
    gate, up = both[:, :hidden], both[:, hidden:]
    act = (gate / (1.0 + jnp.exp(-gate)) * up).astype(BF)
    out_ref[...] = dot(act, down_ref[...]).astype(BF).reshape(out_ref.shape)


def call(kernel, outs, args, flops, in_specs=None, out_specs=None, scratch=(), limit=16):
    moved = sum(a.size * a.dtype.itemsize for a in args)
    shapes = [jax.ShapeDtypeStruct(shape, dtype) for shape, dtype in outs]
    return pl.pallas_call(
        kernel,
        out_shape=shapes,
        in_specs=in_specs or [VMEM] * len(args),
        out_specs=out_specs or [VMEM] * len(shapes),
        scratch_shapes=list(scratch),
        cost_estimate=pl.CostEstimate(flops=flops, bytes_accessed=moved, transcendentals=0),
        compiler_params=pltpu.CompilerParams(vmem_limit_bytes=limit << 20),
    )(*args)


def per_device(
    tokens,
    norm_gain,
    query_weight,
    key_weight,
    value_weight,
    outgate_weight,
    beta_weight,
    decay_weight,
    decay_rate,
    decay_bias,
    head_gain,
    recurrent,
    output_weight,
    ffn_gain,
    routes,
    route_weight,
    expert_gate,
    expert_up,
    expert_down,
    shared_gate,
    shared_up,
    shared_down,
    branch_gate,
):
    nz, ny, nc, _ = (lax.axis_size(a) for a in "zycx")
    ep_count = nz * ny * nc
    seqs, width = tokens.shape
    heads, key_dim, value_dim = recurrent.shape[1:]
    block_k = width // nz
    inner = heads * value_dim

    wo_rows = output_weight.T
    half, rows = seqs // 2, wo_rows.shape[0]
    depth = half + rows + rows // 2 + rows // 4
    pieces = (query_weight, key_weight, value_weight, outgate_weight)
    across = sum(w.shape[1] for w in pieces)
    inputs = (tokens, norm_gain.reshape(width // 128, 128), wo_rows, shared_gate, shared_up, shared_down.T)
    packed, normed, weights = call(
        prep_kernel,
        [((nz, depth, 2 * block_k), BF), ((seqs, width), BF), ((rows, across), BF)],
        inputs + pieces,
        1 << 20,
        in_specs=[HBM] * 10,
        limit=60,
        scratch=[pltpu.VMEM(a.shape, BF) for a in inputs] + [pltpu.SemaphoreType.DMA((10,))],
    )
    arrived = exchange(packed, "z")
    wo_block = arrived[:, half : half + rows]
    shared_block = arrived[:, half + rows :]

    w_own, w_other = around_y_and_c(weights)

    (partial,) = call(
        proj_kernel, [((nz, seqs, weights.shape[1]), BF)], (arrived, w_own, w_other), 1 << 26
    )
    sums = exchange(partial, "z")

    wo_here, wo_below, wo_far, wo_above = around_y(wo_block, nz // 2)
    wo_near = jnp.stack((wo_here, wo_below, wo_above))
    wo_other_near = shifted(wo_near, "c", 1)
    wo_other_far = [shifted(half, "c", 1) for half in wo_far]

    head_start = lax.axis_index("x") * heads
    beta_logit = dot(normed, lax.dynamic_slice_in_dim(beta_weight, head_start, heads, 1))
    decay_logit = dot(normed, lax.dynamic_slice_in_dim(decay_weight, head_start, heads, 1))
    strength = jax.nn.sigmoid(beta_logit)
    retain = jnp.exp(-decay_rate[None, :] * jax.nn.softplus(decay_logit + decay_bias[None, :]))

    new_state, heads_out = call(
        functools.partial(delta_kernel, query_weight.shape[1] // key_dim),
        [(recurrent.shape, F32), ((seqs, inner), BF)],
        (sums, strength, retain, head_gain.reshape(1, value_dim), recurrent),
        1 << 26,
        in_specs=[VMEM, VMEM, VMEM, VMEM, HBM],
        out_specs=[HBM, VMEM],
        limit=52,
        scratch=[
            pltpu.VMEM(recurrent.shape, F32),
            pltpu.VMEM(recurrent.shape, F32),
            pltpu.VMEM((seqs, inner), F32),
            pltpu.SemaphoreType.DMA((seqs,)),
            pltpu.SemaphoreType.DMA((seqs,)),
        ],
    )
    (partial_mix,) = call(
        mix_kernel,
        [((seqs, width), BF)],
        (heads_out, wo_near, wo_other_near, *wo_far, *wo_other_far),
        1 << 25,
    )

    topk = routes.shape[1]
    pair_count = seqs * topk
    capacity = 2 * ((pair_count + ep_count - 1) // ep_count)
    expert_ids = routes.reshape(pair_count)
    onehot = (expert_ids[:, None] == jnp.arange(ep_count)[None, :]).astype(F32)
    earlier = (jnp.arange(pair_count)[:, None] > jnp.arange(pair_count)[None, :]).astype(F32)
    slots = jnp.sum(jnp.dot(earlier, onehot) * onehot, axis=1).astype(jnp.int32)
    target = (expert_ids * capacity + slots).reshape(seqs, topk)
    place = target[:, :, None] == jnp.arange(ep_count * capacity)[None, None, :]
    scaled = route_weight / jnp.sum(route_weight, axis=1, keepdims=True) * ROUTED_SCALE
    dispatch = jnp.any(place, axis=1).astype(BF)
    combine = jnp.sum(jnp.where(place, scaled[:, :, None], 0.0), axis=1)
    combine_high = combine.astype(BF)
    combine_low = (combine - combine_high.astype(F32)).astype(BF)

    residual, ffn_in, outgoing = call(
        post_kernel,
        [((seqs, width), BF), ((seqs, width), BF), ((ep_count, capacity, width), BF)],
        (*total_over_x(partial_mix), tokens, ffn_gain.reshape(1, width), dispatch),
        1 << 24,
    )
    received = exchange(outgoing, ("z", "y", "c")).reshape(-1, width)

    gate_up = jnp.concatenate((expert_gate[0], expert_up[0]), axis=1)
    (partial_rows,) = call(
        expert_kernel,
        [((ep_count, capacity, width), BF)],
        (received, gate_up, expert_down[0]),
        1 << 28,
    )
    returned = exchange(partial_rows, ("z", "y", "c"))
    returned = returned.reshape(-1, width)

    shared_own, shared_other = around_y_and_c(shared_block)
    (shared_part,) = call(
        shared_kernel,
        [((seqs, width), F32)],
        (ffn_in, branch_gate.reshape(1, width), shared_own, shared_other),
        1 << 25,
    )

    moe = dot(jnp.concatenate((combine_high, combine_low), axis=0), returned)
    addend = (moe[:seqs] + moe[seqs:] + shared_part).astype(BF)
    (layer_out,) = call(
        final_kernel, [((seqs, width), BF)], (*total_over_x(addend), residual), 1 << 20
    )
    return (layer_out, new_state)


def solution(mesh):
    ep, tp = mesh.devices.shape
    fine = Mesh(mesh.devices.reshape(ep // 8, 4, 2, tp), ("z", "y", "c", "x"))
    E = ("z", "y", "c")
    return jax.shard_map(
        per_device,
        mesh=fine,
        in_specs=(
            P(E, None),
            P(),
            P(E, "x"),
            P(E, "x"),
            P(E, "x"),
            P(E, "x"),
            P(),
            P(),
            P("x"),
            P("x"),
            P(),
            P(E, "x", None, None),
            P("x", E),
            P(),
            P(E, None),
            P(E, None),
            P(E, None, "x"),
            P(E, None, "x"),
            P(E, "x", None),
            P(E, "x"),
            P(E, "x"),
            P("x", E),
            P(),
        ),
        out_specs=(P(E, None), P(E, "x", None, None)),
        check_vma=False,
    )
```

```python
import functools

import jax
import jax.numpy as jnp
from jax import lax
from jax.experimental import pallas as pl
from jax.experimental.pallas import tpu as pltpu
from jax.sharding import Mesh
from jax.sharding import PartitionSpec as P

EPS = 1e-06
ROUTED_SCALE = 2.5
BF = jnp.bfloat16
F32 = jnp.float32
VMEM = pl.BlockSpec(memory_space=pltpu.VMEM)
HBM = pl.BlockSpec(memory_space=pltpu.HBM)
NT = (((1,), (1,)), ((), ()))


def rms_scale(values, gain):
    values = values.astype(F32)
    return (
        values
        * lax.rsqrt(jnp.mean(values * values, axis=-1, keepdims=True) + EPS)
        * gain.astype(F32)
    )


def unit_rows(values):
    return values * lax.rsqrt(jnp.sum(values * values, axis=-1, keepdims=True) + EPS)


def exchange(pieces, axis):
    return lax.all_to_all(pieces, axis, split_axis=0, concat_axis=0, tiled=True)


def dot(a, b):
    return jnp.dot(a, b, preferred_element_type=F32)


def shifted(array, axis, by):
    n = lax.axis_size(axis)
    return lax.ppermute(array, axis, [(i, (i + by) % n) for i in range(n)])


def around_y(block, cut):
    below = shifted(block, "y", 1)
    above = shifted(block, "y", -1)
    far_low = shifted(below[:cut], "y", 1)
    far_high = shifted(above[cut:], "y", -1)
    return block, below, (far_low, far_high), above


def around_y_and_c(block):
    below = shifted(block, "y", 1)
    above = shifted(block, "y", -1)
    far = shifted(below, "y", 1)
    own = jnp.stack((block, below, far, above))
    return own, shifted(own, "c", 1)


def total_over_x(part):
    return [part] + [shifted(part, "x", i) for i in (2, 1, 3)]


def four(a_ref, b_ref, c_ref, d_ref):
    a, b, c, d = (r[...].astype(F32) for r in (a_ref, b_ref, c_ref, d_ref))
    return (a + b) + (c + d)


def block_of(refs, z, y, c):
    near_ref, other_near_ref, *fars = refs
    at = lax.rem(lax.axis_index("y") - y + 4, 4)
    near = jnp.minimum(at, 2)
    mine = lax.axis_index("c") == c
    here = jnp.where(mine, near_ref[near, z], other_near_ref[near, z])
    half = fars[0].shape[0]
    far = jnp.where(mine, fars[z // half][z % half], fars[2 + z // half][z % half])
    return jnp.where(at == 2, far, here)


def group_rows(refs, group):
    z, first_y = group // 2, 2 * (group % 2)
    return jnp.concatenate(
        [block_of(refs, z, first_y + i // 2, i % 2) for i in range(4)], axis=0
    )


def prep_kernel(*refs):
    sources, (out_ref, normed_ref, weights_ref), targets = refs[:10], refs[10:13], list(refs[13:19])
    tok_ref, gain_ref, wo_ref, gate_ref, up_ref, down_ref = targets
    at = 0
    for source in sources[6:]:
        targets.append(weights_ref.at[:, at : at + source.shape[1]])
        at += source.shape[1]
    moves = [
        pltpu.make_async_copy(source, target, refs[19].at[i])
        for i, (source, target) in enumerate(zip(sources, targets))
    ]
    for move in moves:
        move.start()
    for move in moves[:6]:
        move.wait()
    half = tok_ref.shape[0] // 2
    values = tok_ref[...].astype(F32)
    scale = lax.rsqrt(jnp.mean(values * values, axis=-1, keepdims=True) + EPS)
    gain = gain_ref[...].astype(F32)
    peers, _, wide = out_ref.shape
    cols = wide // 2
    rows, hidden = gate_ref.shape
    for j in range(gain.shape[0]):
        lanes = slice(j * 128, (j + 1) * 128)
        part = (values[:, lanes] * scale * gain[j : j + 1]).astype(BF)
        normed_ref[:, lanes] = part
        z, at = j * 128 // cols, j * 128 % cols
        out_ref[z, 0:half, at : at + 128] = part[:half]
        out_ref[z, 0:half, cols + at : cols + at + 128] = part[half:]
    for z in range(peers):
        at = half
        out_ref[z, at : at + rows, :] = wo_ref[...]
        at += rows
        for i in range(2):
            part = slice(i * rows // 2, (i + 1) * rows // 2)
            out_ref[z, at : at + rows // 2, 2 * i * hidden : (2 * i + 1) * hidden] = gate_ref[part]
            out_ref[z, at : at + rows // 2, (2 * i + 1) * hidden : (2 * i + 2) * hidden] = up_ref[part]
        at += rows // 2
        for i in range(4):
            part = slice(i * rows // 4, (i + 1) * rows // 4)
            out_ref[z, at : at + rows // 4, i * hidden : (i + 1) * hidden] = down_ref[part]
    for move in moves[6:]:
        move.wait()


def proj_kernel(arr_ref, own_ref, other_ref, out_ref):
    peers, seqs, _ = out_ref.shape
    half = seqs // 2
    cols = arr_ref.shape[2] // 2
    parts = []
    for z in range(peers):
        parts += [arr_ref[z, 0:half, 0:cols], arr_ref[z, 0:half, cols : 2 * cols]]
    rows = jnp.concatenate(parts, axis=0)
    me_y, me_c = lax.axis_index("y"), lax.axis_index("c")
    blocks = []
    for i in range(8):
        at = lax.rem(me_y - i // 2 + 4, 4)
        blocks.append(jnp.where(me_c == i % 2, own_ref[at], other_ref[at]))
    part = dot(rows, jnp.concatenate(blocks, axis=0)).astype(BF)
    for z in range(peers):
        out_ref[z] = part[z * seqs : (z + 1) * seqs]


def state_copies(state_hbm, state_ref, sems):
    copies_in = [
        pltpu.make_async_copy(state_hbm.at[s], state_ref.at[s], sems.at[s])
        for s in range(state_ref.shape[0])
    ]
    for copy in copies_in:
        copy.start()
    return copies_in


def delta_kernel(
    key_local, arr_ref, strength_ref, retain_ref, gain_ref, state_hbm, heads_ref, fix_ref, keys_ref,
    state_ref, read_ref, sems,
):
    seqs, heads, key_dim, value_dim = state_ref.shape
    ins = state_copies(state_hbm, state_ref, sems)
    nq, nv = key_local * key_dim, heads * value_dim
    proj = jnp.sum(arr_ref[...].astype(F32), axis=0).astype(BF).astype(F32)
    silu = proj / (1.0 + jnp.exp(-proj))
    queries, keys, both = [], [], []
    for i in range(key_local):
        q = unit_rows(silu[:, i * key_dim : (i + 1) * key_dim]) * key_dim**-0.5
        k = unit_rows(silu[:, nq + i * key_dim : nq + (i + 1) * key_dim])
        both.append(jnp.sum(q * k, axis=1, keepdims=True))
        queries.append(q.T)
        keys.append(k.T)
        keys_ref[i] = k.T
    strength, retain = strength_ref[...], retain_ref[...]
    for s in range(seqs):
        ins[s].wait()
        for h in range(heads):
            i = h * key_local // heads
            row = (slice(s, s + 1), slice(h, h + 1))
            decayed = state_ref[s, h] * retain[row]
            predicted = jnp.sum(decayed * keys[i][:, s : s + 1], axis=0, keepdims=True)
            asked = jnp.sum(decayed * queries[i][:, s : s + 1], axis=0, keepdims=True)
            at = 2 * nq + h * value_dim
            correction = strength[row] * (silu[s : s + 1, at : at + value_dim] - predicted)
            cols = slice(h * value_dim, (h + 1) * value_dim)
            fix_ref[s : s + 1, cols] = correction
            read_ref[s : s + 1, cols] = asked + both[i][s : s + 1] * correction
    for h in range(heads):
        cols = slice(h * value_dim, (h + 1) * value_dim)
        gate = silu[:, 2 * nq + nv + h * value_dim : 2 * nq + nv + (h + 1) * value_dim]
        heads_ref[:, cols] = (rms_scale(read_ref[:, cols], gain_ref[...]) * gate).astype(BF)


def state_kernel(retain_ref, fix_ref, keys_ref, state_hbm, new_hbm, state_ref, new_ref, in_sems, sems):
    seqs, heads, _, value_dim = state_ref.shape
    ins = state_copies(state_hbm, state_ref, in_sems)
    retain = retain_ref[...]
    outs = []
    for s in range(seqs):
        ins[s].wait()
        for h in range(heads):
            kc = keys_ref[h * keys_ref.shape[0] // heads][:, s : s + 1]
            fix = fix_ref[s : s + 1, h * value_dim : (h + 1) * value_dim]
            new_ref[s, h] = state_ref[s, h] * retain[s : s + 1, h : h + 1] + kc * fix
        out = pltpu.make_async_copy(new_ref.at[s], new_hbm.at[s], sems.at[s])
        out.start()
        outs.append(out)
    for out in outs:
        out.wait()


def mix_kernel(heads_ref, *refs):
    heads, out_ref = heads_ref[...], refs[6]
    for group in range(out_ref.shape[1] // 128):
        rows = group_rows(refs[:6], group)
        part = lax.dot_general(heads, rows, NT, preferred_element_type=F32)
        out_ref[:, group * 128 : (group + 1) * 128] = part.astype(BF)


def post_kernel(a_ref, b_ref, c_ref, d_ref, tok_ref, gain_ref, dispatch_ref, res_ref, ffn_ref, out_ref):
    residual = (tok_ref[...].astype(F32) + four(a_ref, b_ref, c_ref, d_ref)).astype(BF)
    res_ref[...] = residual
    ffn_in = rms_scale(residual, gain_ref[...]).astype(BF)
    ffn_ref[...] = ffn_in
    out_ref[...] = lax.dot_general(
        dispatch_ref[...], ffn_in, (((0,), (0,)), ((), ())), preferred_element_type=F32
    ).astype(BF).reshape(out_ref.shape)


def final_kernel(a_ref, b_ref, c_ref, d_ref, res_ref, out_ref):
    out_ref[...] = (res_ref[...].astype(F32) + four(a_ref, b_ref, c_ref, d_ref)).astype(BF)


def shared_kernel(rows_ref, branch_ref, own_ref, other_ref, out_ref):
    groups = out_ref.shape[1] // 128
    hidden = own_ref.shape[3] // 4
    rows = rows_ref[...]
    total = jnp.zeros((rows.shape[0], 2 * hidden), F32)
    downs = []
    for group in range(groups):
        z, first_y = group // 2, 2 * (group % 2)
        block, down = [], []
        for i in range(4):
            at_y = lax.rem(lax.axis_index("y") - first_y - i // 2 + 4, 4)
            mine = lax.axis_index("c") == i % 2
            piece = jnp.where(mine, own_ref[at_y, z], other_ref[at_y, z])
            half = piece.shape[0] * 2 // 3
            block += [piece[:half, : 2 * hidden], piece[:half, 2 * hidden :]]
            down += [piece[half:, j * hidden : (j + 1) * hidden] for j in range(4)]
        downs.append(jnp.concatenate(down, axis=0))
        total += dot(rows[:, group * 128 : (group + 1) * 128], jnp.concatenate(block, axis=0))
    gate, up = total[:, :hidden], total[:, hidden:]
    act = (gate / (1.0 + jnp.exp(-gate)) * up).astype(BF)
    logit = jnp.sum(rows.astype(F32) * branch_ref[...].astype(F32), axis=1, keepdims=True)
    branch = 1.0 / (1.0 + jnp.exp(-logit))
    for group in range(groups):
        part = lax.dot_general(act, downs[group], NT, preferred_element_type=F32)
        out_ref[:, group * 128 : (group + 1) * 128] = branch * part


def expert_kernel(rows_ref, gate_up_ref, down_ref, out_ref):
    both = dot(rows_ref[...], gate_up_ref[...])
    hidden = both.shape[1] // 2
    gate, up = both[:, :hidden], both[:, hidden:]
    act = (gate / (1.0 + jnp.exp(-gate)) * up).astype(BF)
    out_ref[...] = dot(act, down_ref[...]).astype(BF).reshape(out_ref.shape)


def call(kernel, outs, args, flops, in_specs=None, out_specs=None, scratch=(), limit=16):
    moved = sum(a.size * a.dtype.itemsize for a in args)
    shapes = [jax.ShapeDtypeStruct(shape, dtype) for shape, dtype in outs]
    return pl.pallas_call(
        kernel,
        out_shape=shapes,
        in_specs=in_specs or [VMEM] * len(args),
        out_specs=out_specs or [VMEM] * len(shapes),
        scratch_shapes=list(scratch),
        cost_estimate=pl.CostEstimate(flops=flops, bytes_accessed=moved, transcendentals=0),
        compiler_params=pltpu.CompilerParams(vmem_limit_bytes=limit << 20),
    )(*args)


def per_device(
    tokens,
    norm_gain,
    query_weight,
    key_weight,
    value_weight,
    outgate_weight,
    beta_weight,
    decay_weight,
    decay_rate,
    decay_bias,
    head_gain,
    recurrent,
    output_weight,
    ffn_gain,
    routes,
    route_weight,
    expert_gate,
    expert_up,
    expert_down,
    shared_gate,
    shared_up,
    shared_down,
    branch_gate,
):
    nz, ny, nc, _ = (lax.axis_size(a) for a in "zycx")
    ep_count = nz * ny * nc
    seqs, width = tokens.shape
    heads, key_dim, value_dim = recurrent.shape[1:]
    block_k = width // nz
    inner = heads * value_dim

    wo_rows = output_weight.T
    half, rows = seqs // 2, wo_rows.shape[0]
    depth = half + rows + rows // 2 + rows // 4
    pieces = (query_weight, key_weight, value_weight, outgate_weight)
    across = sum(w.shape[1] for w in pieces)
    inputs = (tokens, norm_gain.reshape(width // 128, 128), wo_rows, shared_gate, shared_up, shared_down.T)
    packed, normed, weights = call(
        prep_kernel,
        [((nz, depth, 2 * block_k), BF), ((seqs, width), BF), ((rows, across), BF)],
        inputs + pieces,
        1 << 20,
        in_specs=[HBM] * 10,
        limit=60,
        scratch=[pltpu.VMEM(a.shape, BF) for a in inputs] + [pltpu.SemaphoreType.DMA((10,))],
    )
    arrived = exchange(packed, "z")
    wo_block = arrived[:, half : half + rows]
    shared_block = arrived[:, half + rows :]

    w_own, w_other = around_y_and_c(weights)

    (partial,) = call(
        proj_kernel, [((nz, seqs, weights.shape[1]), BF)], (arrived, w_own, w_other), 1 << 26
    )
    sums = exchange(partial, "z")

    wo_here, wo_below, wo_far, wo_above = around_y(wo_block, nz // 2)
    wo_near = jnp.stack((wo_here, wo_below, wo_above))
    wo_other_near = shifted(wo_near, "c", 1)
    wo_other_far = [shifted(half, "c", 1) for half in wo_far]

    head_start = lax.axis_index("x") * heads
    beta_logit = dot(normed, lax.dynamic_slice_in_dim(beta_weight, head_start, heads, 1))
    decay_logit = dot(normed, lax.dynamic_slice_in_dim(decay_weight, head_start, heads, 1))
    strength = jax.nn.sigmoid(beta_logit)
    retain = jnp.exp(-decay_rate[None, :] * jax.nn.softplus(decay_logit + decay_bias[None, :]))

    key_local = query_weight.shape[1] // key_dim
    heads_out, fixes, keys = call(
        functools.partial(delta_kernel, key_local),
        [((seqs, inner), BF), ((seqs, inner), F32), ((key_local, key_dim, seqs), F32)],
        (sums, strength, retain, head_gain.reshape(1, value_dim), recurrent),
        1 << 26,
        in_specs=[VMEM, VMEM, VMEM, VMEM, HBM],
        limit=52,
        scratch=[
            pltpu.VMEM(recurrent.shape, F32),
            pltpu.VMEM((seqs, inner), F32),
            pltpu.SemaphoreType.DMA((seqs,)),
        ],
    )
    (new_state,) = call(
        state_kernel,
        [(recurrent.shape, F32)],
        (retain, fixes, keys, recurrent),
        1 << 26,
        in_specs=[VMEM, VMEM, VMEM, HBM],
        out_specs=[HBM],
        limit=52,
        scratch=[
            pltpu.VMEM(recurrent.shape, F32),
            pltpu.VMEM(recurrent.shape, F32),
            pltpu.SemaphoreType.DMA((seqs,)),
            pltpu.SemaphoreType.DMA((seqs,)),
        ],
    )
    (partial_mix,) = call(
        mix_kernel,
        [((seqs, width), BF)],
        (heads_out, wo_near, wo_other_near, *wo_far, *wo_other_far),
        1 << 25,
    )

    topk = routes.shape[1]
    pair_count = seqs * topk
    capacity = 2 * ((pair_count + ep_count - 1) // ep_count)
    expert_ids = routes.reshape(pair_count)
    onehot = (expert_ids[:, None] == jnp.arange(ep_count)[None, :]).astype(F32)
    earlier = (jnp.arange(pair_count)[:, None] > jnp.arange(pair_count)[None, :]).astype(F32)
    slots = jnp.sum(jnp.dot(earlier, onehot) * onehot, axis=1).astype(jnp.int32)
    target = (expert_ids * capacity + slots).reshape(seqs, topk)
    place = target[:, :, None] == jnp.arange(ep_count * capacity)[None, None, :]
    scaled = route_weight / jnp.sum(route_weight, axis=1, keepdims=True) * ROUTED_SCALE
    dispatch = jnp.any(place, axis=1).astype(BF)
    combine = jnp.sum(jnp.where(place, scaled[:, :, None], 0.0), axis=1)
    combine_high = combine.astype(BF)
    combine_low = (combine - combine_high.astype(F32)).astype(BF)

    residual, ffn_in, outgoing = call(
        post_kernel,
        [((seqs, width), BF), ((seqs, width), BF), ((ep_count, capacity, width), BF)],
        (*total_over_x(partial_mix), tokens, ffn_gain.reshape(1, width), dispatch),
        1 << 24,
    )
    received = exchange(outgoing, ("z", "y", "c")).reshape(-1, width)

    gate_up = jnp.concatenate((expert_gate[0], expert_up[0]), axis=1)
    (partial_rows,) = call(
        expert_kernel,
        [((ep_count, capacity, width), BF)],
        (received, gate_up, expert_down[0]),
        1 << 28,
    )
    returned = exchange(partial_rows, ("z", "y", "c"))
    returned = returned.reshape(-1, width)

    shared_own, shared_other = around_y_and_c(shared_block)
    (shared_part,) = call(
        shared_kernel,
        [((seqs, width), F32)],
        (ffn_in, branch_gate.reshape(1, width), shared_own, shared_other),
        1 << 25,
    )

    moe = dot(jnp.concatenate((combine_high, combine_low), axis=0), returned)
    addend = (moe[:seqs] + moe[seqs:] + shared_part).astype(BF)
    (layer_out,) = call(
        final_kernel, [((seqs, width), BF)], (*total_over_x(addend), residual), 1 << 20
    )
    return (layer_out, new_state)


def solution(mesh):
    ep, tp = mesh.devices.shape
    fine = Mesh(mesh.devices.reshape(ep // 8, 4, 2, tp), ("z", "y", "c", "x"))
    E = ("z", "y", "c")
    return jax.shard_map(
        per_device,
        mesh=fine,
        in_specs=(
            P(E, None),
            P(),
            P(E, "x"),
            P(E, "x"),
            P(E, "x"),
            P(E, "x"),
            P(),
            P(),
            P("x"),
            P("x"),
            P(),
            P(E, "x", None, None),
            P("x", E),
            P(),
            P(E, None),
            P(E, None),
            P(E, None, "x"),
            P(E, None, "x"),
            P(E, "x", None),
            P(E, "x"),
            P(E, "x"),
            P("x", E),
            P(),
        ),
        out_specs=(P(E, None), P(E, "x", None, None)),
        check_vma=False,
    )
```

```python
import functools

import jax
import jax.numpy as jnp
from jax import lax
from jax.experimental import pallas as pl
from jax.experimental.pallas import tpu as pltpu
from jax.sharding import Mesh
from jax.sharding import PartitionSpec as P

EPS = 1e-06
ROUTED_SCALE = 2.5
BF = jnp.bfloat16
F32 = jnp.float32
VMEM = pl.BlockSpec(memory_space=pltpu.VMEM)
HBM = pl.BlockSpec(memory_space=pltpu.HBM)
NT = (((1,), (1,)), ((), ()))


def rms_scale(values, gain):
    values = values.astype(F32)
    return (
        values
        * lax.rsqrt(jnp.mean(values * values, axis=-1, keepdims=True) + EPS)
        * gain.astype(F32)
    )


def unit_rows(values):
    return values * lax.rsqrt(jnp.sum(values * values, axis=-1, keepdims=True) + EPS)


def exchange(pieces, axis):
    return lax.all_to_all(pieces, axis, split_axis=0, concat_axis=0, tiled=True)


def dot(a, b):
    return jnp.dot(a, b, preferred_element_type=F32)


def shifted(array, axis, by):
    n = lax.axis_size(axis)
    return lax.ppermute(array, axis, [(i, (i + by) % n) for i in range(n)])


def around_y(block, cut):
    below = shifted(block, "y", 1)
    above = shifted(block, "y", -1)
    far_low = shifted(below[:cut], "y", 1)
    far_high = shifted(above[cut:], "y", -1)
    return block, below, (far_low, far_high), above


def around_y_and_c(block):
    below = shifted(block, "y", 1)
    above = shifted(block, "y", -1)
    far = shifted(below, "y", 1)
    own = jnp.stack((block, below, far, above))
    return own, shifted(own, "c", 1)


def total_over_x(part):
    return [part] + [shifted(part, "x", i) for i in (2, 1, 3)]


def four(a_ref, b_ref, c_ref, d_ref):
    a, b, c, d = (r[...].astype(F32) for r in (a_ref, b_ref, c_ref, d_ref))
    return (a + b) + (c + d)


def block_of(refs, z, y, c):
    near_ref, other_near_ref, *fars = refs
    at = lax.rem(lax.axis_index("y") - y + 4, 4)
    near = jnp.minimum(at, 2)
    mine = lax.axis_index("c") == c
    here = jnp.where(mine, near_ref[near, z], other_near_ref[near, z])
    half = fars[0].shape[0]
    far = jnp.where(mine, fars[z // half][z % half], fars[2 + z // half][z % half])
    return jnp.where(at == 2, far, here)


def group_rows(refs, group):
    z, first_y = group // 2, 2 * (group % 2)
    return jnp.concatenate(
        [block_of(refs, z, first_y + i // 2, i % 2) for i in range(4)], axis=0
    )


def prep_kernel(*refs):
    sources, (out_ref, normed_ref, weights_ref), targets = refs[:10], refs[10:13], list(refs[13:19])
    tok_ref, gain_ref, wo_ref, gate_ref, up_ref, down_ref = targets
    at = 0
    for source in sources[6:]:
        targets.append(weights_ref.at[:, at : at + source.shape[1]])
        at += source.shape[1]
    moves = [
        pltpu.make_async_copy(source, target, refs[19].at[i])
        for i, (source, target) in enumerate(zip(sources, targets))
    ]
    for move in moves:
        move.start()
    for move in moves[:6]:
        move.wait()
    half = tok_ref.shape[0] // 2
    values = tok_ref[...].astype(F32)
    scale = lax.rsqrt(jnp.mean(values * values, axis=-1, keepdims=True) + EPS)
    gain = gain_ref[...].astype(F32)
    peers, _, wide = out_ref.shape
    cols = wide // 2
    rows, hidden = gate_ref.shape
    for j in range(gain.shape[0]):
        lanes = slice(j * 128, (j + 1) * 128)
        part = (values[:, lanes] * scale * gain[j : j + 1]).astype(BF)
        normed_ref[:, lanes] = part
        z, at = j * 128 // cols, j * 128 % cols
        out_ref[z, 0:half, at : at + 128] = part[:half]
        out_ref[z, 0:half, cols + at : cols + at + 128] = part[half:]
    for z in range(peers):
        at = half
        out_ref[z, at : at + rows, :] = wo_ref[...]
        at += rows
        for i in range(2):
            part = slice(i * rows // 2, (i + 1) * rows // 2)
            out_ref[z, at : at + rows // 2, 2 * i * hidden : (2 * i + 1) * hidden] = gate_ref[part]
            out_ref[z, at : at + rows // 2, (2 * i + 1) * hidden : (2 * i + 2) * hidden] = up_ref[part]
        at += rows // 2
        for i in range(4):
            part = slice(i * rows // 4, (i + 1) * rows // 4)
            out_ref[z, at : at + rows // 4, i * hidden : (i + 1) * hidden] = down_ref[part]
    for move in moves[6:]:
        move.wait()


def proj_kernel(arr_ref, own_ref, other_ref, out_ref):
    peers, seqs, _ = out_ref.shape
    half = seqs // 2
    cols = arr_ref.shape[2] // 2
    parts = []
    for z in range(peers):
        parts += [arr_ref[z, 0:half, 0:cols], arr_ref[z, 0:half, cols : 2 * cols]]
    rows = jnp.concatenate(parts, axis=0)
    me_y, me_c = lax.axis_index("y"), lax.axis_index("c")
    blocks = []
    for i in range(8):
        at = lax.rem(me_y - i // 2 + 4, 4)
        blocks.append(jnp.where(me_c == i % 2, own_ref[at], other_ref[at]))
    part = dot(rows, jnp.concatenate(blocks, axis=0)).astype(BF)
    for z in range(peers):
        out_ref[z] = part[z * seqs : (z + 1) * seqs]


def state_copies(state_hbm, state_ref, sems):
    return [
        pltpu.make_async_copy(state_hbm.at[s], state_ref.at[s], sems.at[s])
        for s in range(state_ref.shape[0])
    ]


def delta_kernel(
    key_local, arr_ref, strength_ref, retain_ref, gain_ref, state_hbm, heads_ref, fix_ref, keys_ref,
    state_ref, read_ref, sems,
):
    seqs, heads, key_dim, value_dim = state_ref.shape
    ins = state_copies(state_hbm, state_ref, sems)
    for copy in ins[:3]:
        copy.start()
    nq, nv = key_local * key_dim, heads * value_dim
    proj = jnp.sum(arr_ref[...].astype(F32), axis=0).astype(BF).astype(F32)
    silu = proj / (1.0 + jnp.exp(-proj))
    queries, keys, both = [], [], []
    for i in range(key_local):
        q = unit_rows(silu[:, i * key_dim : (i + 1) * key_dim]) * key_dim**-0.5
        k = unit_rows(silu[:, nq + i * key_dim : nq + (i + 1) * key_dim])
        both.append(jnp.sum(q * k, axis=1, keepdims=True))
        queries.append(q.T)
        keys.append(k.T)
        keys_ref[i] = k.T
    strength, retain = strength_ref[...], retain_ref[...]
    for copy in ins[3:]:
        copy.start()
    for s in range(seqs):
        ins[s].wait()
        for h in range(heads):
            i = h * key_local // heads
            row = (slice(s, s + 1), slice(h, h + 1))
            state = state_ref[s, h]
            predicted = jnp.sum(state * keys[i][:, s : s + 1], axis=0, keepdims=True)
            asked = jnp.sum(state * queries[i][:, s : s + 1], axis=0, keepdims=True)
            at = 2 * nq + h * value_dim
            value = silu[s : s + 1, at : at + value_dim]
            correction = strength[row] * (value - retain[row] * predicted)
            cols = slice(h * value_dim, (h + 1) * value_dim)
            fix_ref[s : s + 1, cols] = correction
            read_ref[s : s + 1, cols] = retain[row] * asked + both[i][s : s + 1] * correction
    for h in range(heads):
        cols = slice(h * value_dim, (h + 1) * value_dim)
        gate = silu[:, 2 * nq + nv + h * value_dim : 2 * nq + nv + (h + 1) * value_dim]
        heads_ref[:, cols] = (rms_scale(read_ref[:, cols], gain_ref[...]) * gate).astype(BF)


def state_kernel(retain_ref, fix_ref, keys_ref, state_hbm, new_hbm, state_ref, new_ref, in_sems, sems):
    seqs, heads, _, value_dim = state_ref.shape
    ins = state_copies(state_hbm, state_ref, in_sems)
    for copy in ins:
        copy.start()
    retain = retain_ref[...]
    outs = []
    for s in range(seqs):
        ins[s].wait()
        for h in range(heads):
            kc = keys_ref[h * keys_ref.shape[0] // heads][:, s : s + 1]
            fix = fix_ref[s : s + 1, h * value_dim : (h + 1) * value_dim]
            new_ref[s, h] = state_ref[s, h] * retain[s : s + 1, h : h + 1] + kc * fix
        out = pltpu.make_async_copy(new_ref.at[s], new_hbm.at[s], sems.at[s])
        out.start()
        outs.append(out)
    for out in outs:
        out.wait()


def mix_kernel(heads_ref, *refs):
    heads, out_ref = heads_ref[...], refs[6]
    for group in range(out_ref.shape[1] // 128):
        rows = group_rows(refs[:6], group)
        part = lax.dot_general(heads, rows, NT, preferred_element_type=F32)
        out_ref[:, group * 128 : (group + 1) * 128] = part.astype(BF)


def post_kernel(a_ref, b_ref, c_ref, d_ref, tok_ref, gain_ref, dispatch_ref, res_ref, ffn_ref, out_ref):
    residual = (tok_ref[...].astype(F32) + four(a_ref, b_ref, c_ref, d_ref)).astype(BF)
    res_ref[...] = residual
    ffn_in = rms_scale(residual, gain_ref[...]).astype(BF)
    ffn_ref[...] = ffn_in
    out_ref[...] = lax.dot_general(
        dispatch_ref[...], ffn_in, (((0,), (0,)), ((), ())), preferred_element_type=F32
    ).astype(BF).reshape(out_ref.shape)


def final_kernel(a_ref, b_ref, c_ref, d_ref, res_ref, out_ref):
    out_ref[...] = (res_ref[...].astype(F32) + four(a_ref, b_ref, c_ref, d_ref)).astype(BF)


def shared_kernel(rows_ref, branch_ref, own_ref, other_ref, out_ref):
    groups = out_ref.shape[1] // 128
    hidden = own_ref.shape[3] // 4
    rows = rows_ref[...]
    total = jnp.zeros((rows.shape[0], 2 * hidden), F32)
    downs = []
    for group in range(groups):
        z, first_y = group // 2, 2 * (group % 2)
        block, down = [], []
        for i in range(4):
            at_y = lax.rem(lax.axis_index("y") - first_y - i // 2 + 4, 4)
            mine = lax.axis_index("c") == i % 2
            piece = jnp.where(mine, own_ref[at_y, z], other_ref[at_y, z])
            half = piece.shape[0] * 2 // 3
            block += [piece[:half, : 2 * hidden], piece[:half, 2 * hidden :]]
            down += [piece[half:, j * hidden : (j + 1) * hidden] for j in range(4)]
        downs.append(jnp.concatenate(down, axis=0))
        total += dot(rows[:, group * 128 : (group + 1) * 128], jnp.concatenate(block, axis=0))
    gate, up = total[:, :hidden], total[:, hidden:]
    act = (gate / (1.0 + jnp.exp(-gate)) * up).astype(BF)
    logit = jnp.sum(rows.astype(F32) * branch_ref[...].astype(F32), axis=1, keepdims=True)
    branch = 1.0 / (1.0 + jnp.exp(-logit))
    for group in range(groups):
        part = lax.dot_general(act, downs[group], NT, preferred_element_type=F32)
        out_ref[:, group * 128 : (group + 1) * 128] = branch * part


def expert_kernel(rows_ref, gate_up_ref, down_ref, out_ref):
    both = dot(rows_ref[...], gate_up_ref[...])
    hidden = both.shape[1] // 2
    gate, up = both[:, :hidden], both[:, hidden:]
    act = (gate / (1.0 + jnp.exp(-gate)) * up).astype(BF)
    out_ref[...] = dot(act, down_ref[...]).astype(BF).reshape(out_ref.shape)


def call(kernel, outs, args, flops, in_specs=None, out_specs=None, scratch=(), limit=16):
    moved = sum(a.size * a.dtype.itemsize for a in args)
    shapes = [jax.ShapeDtypeStruct(shape, dtype) for shape, dtype in outs]
    return pl.pallas_call(
        kernel,
        out_shape=shapes,
        in_specs=in_specs or [VMEM] * len(args),
        out_specs=out_specs or [VMEM] * len(shapes),
        scratch_shapes=list(scratch),
        cost_estimate=pl.CostEstimate(flops=flops, bytes_accessed=moved, transcendentals=0),
        compiler_params=pltpu.CompilerParams(vmem_limit_bytes=limit << 20),
    )(*args)


def per_device(
    tokens,
    norm_gain,
    query_weight,
    key_weight,
    value_weight,
    outgate_weight,
    beta_weight,
    decay_weight,
    decay_rate,
    decay_bias,
    head_gain,
    recurrent,
    output_weight,
    ffn_gain,
    routes,
    route_weight,
    expert_gate,
    expert_up,
    expert_down,
    shared_gate,
    shared_up,
    shared_down,
    branch_gate,
):
    nz, ny, nc, _ = (lax.axis_size(a) for a in "zycx")
    ep_count = nz * ny * nc
    seqs, width = tokens.shape
    heads, key_dim, value_dim = recurrent.shape[1:]
    block_k = width // nz
    inner = heads * value_dim

    wo_rows = output_weight.T
    half, rows = seqs // 2, wo_rows.shape[0]
    depth = half + rows + rows // 2 + rows // 4
    pieces = (query_weight, key_weight, value_weight, outgate_weight)
    across = sum(w.shape[1] for w in pieces)
    inputs = (tokens, norm_gain.reshape(width // 128, 128), wo_rows, shared_gate, shared_up, shared_down.T)
    packed, normed, weights = call(
        prep_kernel,
        [((nz, depth, 2 * block_k), BF), ((seqs, width), BF), ((rows, across), BF)],
        inputs + pieces,
        1 << 20,
        in_specs=[HBM] * 10,
        limit=60,
        scratch=[pltpu.VMEM(a.shape, BF) for a in inputs] + [pltpu.SemaphoreType.DMA((10,))],
    )
    arrived = exchange(packed, "z")
    wo_block = arrived[:, half : half + rows]
    shared_block = arrived[:, half + rows :]

    w_own, w_other = around_y_and_c(weights)

    (partial,) = call(
        proj_kernel, [((nz, seqs, weights.shape[1]), BF)], (arrived, w_own, w_other), 1 << 26
    )
    sums = exchange(partial, "z")

    wo_here, wo_below, wo_far, wo_above = around_y(wo_block, nz // 2)
    wo_near = jnp.stack((wo_here, wo_below, wo_above))
    wo_other_near = shifted(wo_near, "c", 1)
    wo_other_far = [shifted(half, "c", 1) for half in wo_far]

    head_start = lax.axis_index("x") * heads
    beta_logit = dot(normed, lax.dynamic_slice_in_dim(beta_weight, head_start, heads, 1))
    decay_logit = dot(normed, lax.dynamic_slice_in_dim(decay_weight, head_start, heads, 1))
    strength = jax.nn.sigmoid(beta_logit)
    retain = jnp.exp(-decay_rate[None, :] * jax.nn.softplus(decay_logit + decay_bias[None, :]))

    key_local = query_weight.shape[1] // key_dim
    heads_out, fixes, keys = call(
        functools.partial(delta_kernel, key_local),
        [((seqs, inner), BF), ((seqs, inner), F32), ((key_local, key_dim, seqs), F32)],
        (sums, strength, retain, head_gain.reshape(1, value_dim), recurrent),
        1 << 26,
        in_specs=[VMEM, VMEM, VMEM, VMEM, HBM],
        limit=52,
        scratch=[
            pltpu.VMEM(recurrent.shape, F32),
            pltpu.VMEM((seqs, inner), F32),
            pltpu.SemaphoreType.DMA((seqs,)),
        ],
    )
    (new_state,) = call(
        state_kernel,
        [(recurrent.shape, F32)],
        (retain, fixes, keys, recurrent),
        1 << 26,
        in_specs=[VMEM, VMEM, VMEM, HBM],
        out_specs=[HBM],
        limit=52,
        scratch=[
            pltpu.VMEM(recurrent.shape, F32),
            pltpu.VMEM(recurrent.shape, F32),
            pltpu.SemaphoreType.DMA((seqs,)),
            pltpu.SemaphoreType.DMA((seqs,)),
        ],
    )
    (partial_mix,) = call(
        mix_kernel,
        [((seqs, width), BF)],
        (heads_out, wo_near, wo_other_near, *wo_far, *wo_other_far),
        1 << 25,
    )

    topk = routes.shape[1]
    pair_count = seqs * topk
    capacity = 2 * ((pair_count + ep_count - 1) // ep_count)
    expert_ids = routes.reshape(pair_count)
    onehot = (expert_ids[:, None] == jnp.arange(ep_count)[None, :]).astype(F32)
    earlier = (jnp.arange(pair_count)[:, None] > jnp.arange(pair_count)[None, :]).astype(F32)
    slots = jnp.sum(jnp.dot(earlier, onehot) * onehot, axis=1).astype(jnp.int32)
    target = (expert_ids * capacity + slots).reshape(seqs, topk)
    place = target[:, :, None] == jnp.arange(ep_count * capacity)[None, None, :]
    scaled = route_weight / jnp.sum(route_weight, axis=1, keepdims=True) * ROUTED_SCALE
    dispatch = jnp.any(place, axis=1).astype(BF)
    combine = jnp.sum(jnp.where(place, scaled[:, :, None], 0.0), axis=1)
    combine_high = combine.astype(BF)
    combine_low = (combine - combine_high.astype(F32)).astype(BF)

    residual, ffn_in, outgoing = call(
        post_kernel,
        [((seqs, width), BF), ((seqs, width), BF), ((ep_count, capacity, width), BF)],
        (*total_over_x(partial_mix), tokens, ffn_gain.reshape(1, width), dispatch),
        1 << 24,
    )
    received = exchange(outgoing, ("z", "y", "c")).reshape(-1, width)

    gate_up = jnp.concatenate((expert_gate[0], expert_up[0]), axis=1)
    (partial_rows,) = call(
        expert_kernel,
        [((ep_count, capacity, width), BF)],
        (received, gate_up, expert_down[0]),
        1 << 28,
    )
    returned = exchange(partial_rows, ("z", "y", "c"))
    returned = returned.reshape(-1, width)

    shared_own, shared_other = around_y_and_c(shared_block)
    (shared_part,) = call(
        shared_kernel,
        [((seqs, width), F32)],
        (ffn_in, branch_gate.reshape(1, width), shared_own, shared_other),
        1 << 25,
    )

    moe = dot(jnp.concatenate((combine_high, combine_low), axis=0), returned)
    addend = (moe[:seqs] + moe[seqs:] + shared_part).astype(BF)
    (layer_out,) = call(
        final_kernel, [((seqs, width), BF)], (*total_over_x(addend), residual), 1 << 20
    )
    return (layer_out, new_state)


def solution(mesh):
    ep, tp = mesh.devices.shape
    fine = Mesh(mesh.devices.reshape(ep // 8, 4, 2, tp), ("z", "y", "c", "x"))
    E = ("z", "y", "c")
    return jax.shard_map(
        per_device,
        mesh=fine,
        in_specs=(
            P(E, None),
            P(),
            P(E, "x"),
            P(E, "x"),
            P(E, "x"),
            P(E, "x"),
            P(),
            P(),
            P("x"),
            P("x"),
            P(),
            P(E, "x", None, None),
            P("x", E),
            P(),
            P(E, None),
            P(E, None),
            P(E, None, "x"),
            P(E, None, "x"),
            P(E, "x", None),
            P(E, "x"),
            P(E, "x"),
            P("x", E),
            P(),
        ),
        out_specs=(P(E, None), P(E, "x", None, None)),
        check_vma=False,
    )
```

```python
import functools

import jax
import jax.numpy as jnp
from jax import lax
from jax.experimental import pallas as pl
from jax.experimental.pallas import tpu as pltpu
from jax.sharding import Mesh
from jax.sharding import PartitionSpec as P

EPS = 1e-06
ROUTED_SCALE = 2.5
BF = jnp.bfloat16
F32 = jnp.float32
VMEM = pl.BlockSpec(memory_space=pltpu.VMEM)
HBM = pl.BlockSpec(memory_space=pltpu.HBM)
NT = (((1,), (1,)), ((), ()))


def rms_scale(values, gain):
    values = values.astype(F32)
    return (
        values
        * lax.rsqrt(jnp.mean(values * values, axis=-1, keepdims=True) + EPS)
        * gain.astype(F32)
    )


def unit_rows(values):
    return values * lax.rsqrt(jnp.sum(values * values, axis=-1, keepdims=True) + EPS)


def exchange(pieces, axis):
    return lax.all_to_all(pieces, axis, split_axis=0, concat_axis=0, tiled=True)


def dot(a, b):
    return jnp.dot(a, b, preferred_element_type=F32)


def shifted(array, axis, by):
    n = lax.axis_size(axis)
    return lax.ppermute(array, axis, [(i, (i + by) % n) for i in range(n)])


def around_y(block, cut):
    below = shifted(block, "y", 1)
    above = shifted(block, "y", -1)
    far_low = shifted(below[:cut], "y", 1)
    far_high = shifted(above[cut:], "y", -1)
    return block, below, (far_low, far_high), above


def around_y_and_c(block):
    below = shifted(block, "y", 1)
    above = shifted(block, "y", -1)
    far = shifted(below, "y", 1)
    own = jnp.stack((block, below, far, above))
    return own, shifted(own, "c", 1)


def around_z(block, cut):
    ups, downs = [block], [block]
    for _ in range(1, 4):
        ups.append(shifted(ups[-1], "z", 1))
        downs.append(shifted(downs[-1], "z", -1))
    low = shifted(ups[-1][:cut], "z", 1)
    high = shifted(downs[-1][cut:], "z", -1)
    return (*ups, low, high, *downs[:0:-1])


def total_over_x(part):
    return [part] + [shifted(part, "x", i) for i in (2, 1, 3)]


def four(a_ref, b_ref, c_ref, d_ref):
    a, b, c, d = (r[...].astype(F32) for r in (a_ref, b_ref, c_ref, d_ref))
    return (a + b) + (c + d)


def block_of(refs, z, y, c):
    near_ref, other_near_ref, *fars = refs
    at = lax.rem(lax.axis_index("y") - y + 4, 4)
    near = jnp.minimum(at, 2)
    mine = lax.axis_index("c") == c
    here = jnp.where(mine, near_ref[near, z], other_near_ref[near, z])
    half = fars[0].shape[0]
    far = jnp.where(mine, fars[z // half][z % half], fars[2 + z // half][z % half])
    return jnp.where(at == 2, far, here)


def group_rows(refs, group):
    z, first_y = group // 2, 2 * (group % 2)
    return jnp.concatenate(
        [block_of(refs, z, first_y + i // 2, i % 2) for i in range(4)], axis=0
    )


def prep_kernel(*refs):
    sources, (out_ref, normed_ref, weights_ref, shared_ref) = refs[:10], refs[10:14]
    targets = list(refs[14:20])
    tok_ref, gain_ref, wo_ref, gate_ref, up_ref, down_ref = targets
    at = 0
    for source in sources[6:]:
        targets.append(weights_ref.at[:, at : at + source.shape[1]])
        at += source.shape[1]
    moves = [
        pltpu.make_async_copy(source, target, refs[20].at[i])
        for i, (source, target) in enumerate(zip(sources, targets))
    ]
    for move in moves:
        move.start()
    for move in moves[:6]:
        move.wait()
    half = tok_ref.shape[0] // 2
    values = tok_ref[...].astype(F32)
    scale = lax.rsqrt(jnp.mean(values * values, axis=-1, keepdims=True) + EPS)
    gain = gain_ref[...].astype(F32)
    peers, _, wide = out_ref.shape
    cols = wide // 2
    rows, hidden = gate_ref.shape
    for j in range(gain.shape[0]):
        lanes = slice(j * 128, (j + 1) * 128)
        part = (values[:, lanes] * scale * gain[j : j + 1]).astype(BF)
        normed_ref[:, lanes] = part
        z, at = j * 128 // cols, j * 128 % cols
        out_ref[z, 0:half, at : at + 128] = part[:half]
        out_ref[z, 0:half, cols + at : cols + at + 128] = part[half:]
    for z in range(peers):
        out_ref[z, half : half + rows, :] = wo_ref[...]
    for i in range(2):
        part = slice(i * rows // 2, (i + 1) * rows // 2)
        shared_ref[0 : rows // 2, 2 * i * hidden : (2 * i + 1) * hidden] = gate_ref[part]
        shared_ref[0 : rows // 2, (2 * i + 1) * hidden : (2 * i + 2) * hidden] = up_ref[part]
    for i in range(4):
        part = slice(i * rows // 4, (i + 1) * rows // 4)
        shared_ref[rows // 2 :, i * hidden : (i + 1) * hidden] = down_ref[part]
    for move in moves[6:]:
        move.wait()


def stack_kernel(*refs):
    pieces, out_ref = refs[:9], refs[9]
    cut = pieces[4].shape[0]
    for i, piece in enumerate(pieces[:4] + pieces[6:]):
        out_ref[i + (i > 3)] = piece[...]
    out_ref[4, 0:cut] = pieces[4][...]
    out_ref[4, cut:] = pieces[5][...]


def proj_kernel(arr_ref, own_ref, other_ref, out_ref):
    peers, seqs, _ = out_ref.shape
    half = seqs // 2
    cols = arr_ref.shape[2] // 2
    parts = []
    for z in range(peers):
        parts += [arr_ref[z, 0:half, 0:cols], arr_ref[z, 0:half, cols : 2 * cols]]
    rows = jnp.concatenate(parts, axis=0)
    me_y, me_c = lax.axis_index("y"), lax.axis_index("c")
    blocks = []
    for i in range(8):
        at = lax.rem(me_y - i // 2 + 4, 4)
        blocks.append(jnp.where(me_c == i % 2, own_ref[at], other_ref[at]))
    part = dot(rows, jnp.concatenate(blocks, axis=0)).astype(BF)
    for z in range(peers):
        out_ref[z] = part[z * seqs : (z + 1) * seqs]


def state_copies(state_hbm, state_ref, sems):
    return [
        pltpu.make_async_copy(state_hbm.at[s], state_ref.at[s], sems.at[s])
        for s in range(state_ref.shape[0])
    ]


def delta_kernel(
    key_local, arr_ref, strength_ref, retain_ref, gain_ref, state_hbm, heads_ref, fix_ref, keys_ref,
    state_ref, read_ref, sems,
):
    seqs, heads, key_dim, value_dim = state_ref.shape
    ins = state_copies(state_hbm, state_ref, sems)
    for copy in ins[:3]:
        copy.start()
    nq, nv = key_local * key_dim, heads * value_dim
    proj = jnp.sum(arr_ref[...].astype(F32), axis=0).astype(BF).astype(F32)
    silu = proj / (1.0 + jnp.exp(-proj))
    queries, keys, both = [], [], []
    for i in range(key_local):
        q = unit_rows(silu[:, i * key_dim : (i + 1) * key_dim]) * key_dim**-0.5
        k = unit_rows(silu[:, nq + i * key_dim : nq + (i + 1) * key_dim])
        both.append(jnp.sum(q * k, axis=1, keepdims=True))
        queries.append(q.T)
        keys.append(k.T)
        keys_ref[i] = k.T
    strength, retain = strength_ref[...], retain_ref[...]
    for copy in ins[3:]:
        copy.start()
    for s in range(seqs):
        ins[s].wait()
        for h in range(heads):
            i = h * key_local // heads
            row = (slice(s, s + 1), slice(h, h + 1))
            state = state_ref[s, h]
            predicted = jnp.sum(state * keys[i][:, s : s + 1], axis=0, keepdims=True)
            asked = jnp.sum(state * queries[i][:, s : s + 1], axis=0, keepdims=True)
            at = 2 * nq + h * value_dim
            value = silu[s : s + 1, at : at + value_dim]
            correction = strength[row] * (value - retain[row] * predicted)
            cols = slice(h * value_dim, (h + 1) * value_dim)
            fix_ref[s : s + 1, cols] = correction
            read_ref[s : s + 1, cols] = retain[row] * asked + both[i][s : s + 1] * correction
    for h in range(heads):
        cols = slice(h * value_dim, (h + 1) * value_dim)
        gate = silu[:, 2 * nq + nv + h * value_dim : 2 * nq + nv + (h + 1) * value_dim]
        heads_ref[:, cols] = (rms_scale(read_ref[:, cols], gain_ref[...]) * gate).astype(BF)


def state_kernel(retain_ref, fix_ref, keys_ref, state_hbm, new_hbm, state_ref, new_ref, in_sems, sems):
    seqs, heads, _, value_dim = state_ref.shape
    ins = state_copies(state_hbm, state_ref, in_sems)
    for copy in ins:
        copy.start()
    retain = retain_ref[...]
    outs = []
    for s in range(seqs):
        ins[s].wait()
        for h in range(heads):
            kc = keys_ref[h * keys_ref.shape[0] // heads][:, s : s + 1]
            fix = fix_ref[s : s + 1, h * value_dim : (h + 1) * value_dim]
            new_ref[s, h] = state_ref[s, h] * retain[s : s + 1, h : h + 1] + kc * fix
        out = pltpu.make_async_copy(new_ref.at[s], new_hbm.at[s], sems.at[s])
        out.start()
        outs.append(out)
    for out in outs:
        out.wait()


def mix_kernel(heads_ref, *refs):
    heads, out_ref = heads_ref[...], refs[6]
    for group in range(out_ref.shape[1] // 128):
        rows = group_rows(refs[:6], group)
        part = lax.dot_general(heads, rows, NT, preferred_element_type=F32)
        out_ref[:, group * 128 : (group + 1) * 128] = part.astype(BF)


def post_kernel(a_ref, b_ref, c_ref, d_ref, tok_ref, gain_ref, dispatch_ref, res_ref, ffn_ref, out_ref):
    residual = (tok_ref[...].astype(F32) + four(a_ref, b_ref, c_ref, d_ref)).astype(BF)
    res_ref[...] = residual
    ffn_in = rms_scale(residual, gain_ref[...]).astype(BF)
    ffn_ref[...] = ffn_in
    out_ref[...] = lax.dot_general(
        dispatch_ref[...], ffn_in, (((0,), (0,)), ((), ())), preferred_element_type=F32
    ).astype(BF).reshape(out_ref.shape)


def final_kernel(a_ref, b_ref, c_ref, d_ref, res_ref, out_ref):
    out_ref[...] = (res_ref[...].astype(F32) + four(a_ref, b_ref, c_ref, d_ref)).astype(BF)


def shared_kernel(rows_ref, branch_ref, own_ref, other_ref, out_ref):
    groups = out_ref.shape[1] // 128
    hidden = own_ref.shape[3] // 4
    rows = rows_ref[...]
    total = jnp.zeros((rows.shape[0], 2 * hidden), F32)
    downs = []
    for group in range(groups):
        z, first_y = group // 2, 2 * (group % 2)
        block, down = [], []
        for i in range(4):
            at_y = lax.rem(lax.axis_index("y") - first_y - i // 2 + 4, 4)
            at_z = lax.rem(lax.axis_index("z") - z + 8, 8)
            mine = lax.axis_index("c") == i % 2
            piece = jnp.where(mine, own_ref[at_y, at_z], other_ref[at_y, at_z])
            half = piece.shape[0] * 2 // 3
            block += [piece[:half, : 2 * hidden], piece[:half, 2 * hidden :]]
            down += [piece[half:, j * hidden : (j + 1) * hidden] for j in range(4)]
        downs.append(jnp.concatenate(down, axis=0))
        total += dot(rows[:, group * 128 : (group + 1) * 128], jnp.concatenate(block, axis=0))
    gate, up = total[:, :hidden], total[:, hidden:]
    act = (gate / (1.0 + jnp.exp(-gate)) * up).astype(BF)
    logit = jnp.sum(rows.astype(F32) * branch_ref[...].astype(F32), axis=1, keepdims=True)
    branch = 1.0 / (1.0 + jnp.exp(-logit))
    for group in range(groups):
        part = lax.dot_general(act, downs[group], NT, preferred_element_type=F32)
        out_ref[:, group * 128 : (group + 1) * 128] = branch * part


def expert_kernel(rows_ref, gate_up_ref, down_ref, out_ref):
    both = dot(rows_ref[...], gate_up_ref[...])
    hidden = both.shape[1] // 2
    gate, up = both[:, :hidden], both[:, hidden:]
    act = (gate / (1.0 + jnp.exp(-gate)) * up).astype(BF)
    out_ref[...] = dot(act, down_ref[...]).astype(BF).reshape(out_ref.shape)


def call(kernel, outs, args, flops, in_specs=None, out_specs=None, scratch=(), limit=16):
    moved = sum(a.size * a.dtype.itemsize for a in args)
    shapes = [jax.ShapeDtypeStruct(shape, dtype) for shape, dtype in outs]
    return pl.pallas_call(
        kernel,
        out_shape=shapes,
        in_specs=in_specs or [VMEM] * len(args),
        out_specs=out_specs or [VMEM] * len(shapes),
        scratch_shapes=list(scratch),
        cost_estimate=pl.CostEstimate(flops=flops, bytes_accessed=moved, transcendentals=0),
        compiler_params=pltpu.CompilerParams(vmem_limit_bytes=limit << 20),
    )(*args)


def per_device(
    tokens,
    norm_gain,
    query_weight,
    key_weight,
    value_weight,
    outgate_weight,
    beta_weight,
    decay_weight,
    decay_rate,
    decay_bias,
    head_gain,
    recurrent,
    output_weight,
    ffn_gain,
    routes,
    route_weight,
    expert_gate,
    expert_up,
    expert_down,
    shared_gate,
    shared_up,
    shared_down,
    branch_gate,
):
    nz, ny, nc, _ = (lax.axis_size(a) for a in "zycx")
    ep_count = nz * ny * nc
    seqs, width = tokens.shape
    heads, key_dim, value_dim = recurrent.shape[1:]
    block_k = width // nz
    inner = heads * value_dim

    wo_rows = output_weight.T
    half, rows = seqs // 2, wo_rows.shape[0]
    depth = rows // 2 + rows // 4
    pieces = (query_weight, key_weight, value_weight, outgate_weight)
    across = sum(w.shape[1] for w in pieces)
    inputs = (tokens, norm_gain.reshape(width // 128, 128), wo_rows, shared_gate, shared_up, shared_down.T)
    packed, normed, weights, shared_piece = call(
        prep_kernel,
        [
            ((nz, half + rows, 2 * block_k), BF),
            ((seqs, width), BF),
            ((rows, across), BF),
            ((depth, 4 * shared_gate.shape[1]), BF),
        ],
        inputs + pieces,
        1 << 20,
        in_specs=[HBM] * 10,
        limit=60,
        scratch=[pltpu.VMEM(a.shape, BF) for a in inputs] + [pltpu.SemaphoreType.DMA((10,))],
    )
    arrived = exchange(packed, "z")
    wo_block = arrived[:, half:]
    shared_pieces = around_z(shared_piece, rows // 2)
    (shared_block,) = call(stack_kernel, [((nz, *shared_piece.shape), BF)], shared_pieces, 1 << 20)

    w_own, w_other = around_y_and_c(weights)

    (partial,) = call(
        proj_kernel, [((nz, seqs, weights.shape[1]), BF)], (arrived, w_own, w_other), 1 << 26
    )
    sums = exchange(partial, "z")

    wo_here, wo_below, wo_far, wo_above = around_y(wo_block, nz // 2)
    wo_near = jnp.stack((wo_here, wo_below, wo_above))
    wo_other_near = shifted(wo_near, "c", 1)
    wo_other_far = [shifted(half, "c", 1) for half in wo_far]

    head_start = lax.axis_index("x") * heads
    beta_logit = dot(normed, lax.dynamic_slice_in_dim(beta_weight, head_start, heads, 1))
    decay_logit = dot(normed, lax.dynamic_slice_in_dim(decay_weight, head_start, heads, 1))
    strength = jax.nn.sigmoid(beta_logit)
    retain = jnp.exp(-decay_rate[None, :] * jax.nn.softplus(decay_logit + decay_bias[None, :]))

    key_local = query_weight.shape[1] // key_dim
    heads_out, fixes, keys = call(
        functools.partial(delta_kernel, key_local),
        [((seqs, inner), BF), ((seqs, inner), F32), ((key_local, key_dim, seqs), F32)],
        (sums, strength, retain, head_gain.reshape(1, value_dim), recurrent),
        1 << 26,
        in_specs=[VMEM, VMEM, VMEM, VMEM, HBM],
        limit=52,
        scratch=[
            pltpu.VMEM(recurrent.shape, F32),
            pltpu.VMEM((seqs, inner), F32),
            pltpu.SemaphoreType.DMA((seqs,)),
        ],
    )
    (new_state,) = call(
        state_kernel,
        [(recurrent.shape, F32)],
        (retain, fixes, keys, recurrent),
        1 << 26,
        in_specs=[VMEM, VMEM, VMEM, HBM],
        out_specs=[HBM],
        limit=52,
        scratch=[
            pltpu.VMEM(recurrent.shape, F32),
            pltpu.VMEM(recurrent.shape, F32),
            pltpu.SemaphoreType.DMA((seqs,)),
            pltpu.SemaphoreType.DMA((seqs,)),
        ],
    )
    (partial_mix,) = call(
        mix_kernel,
        [((seqs, width), BF)],
        (heads_out, wo_near, wo_other_near, *wo_far, *wo_other_far),
        1 << 25,
    )

    topk = routes.shape[1]
    pair_count = seqs * topk
    capacity = 2 * ((pair_count + ep_count - 1) // ep_count)
    expert_ids = routes.reshape(pair_count)
    onehot = (expert_ids[:, None] == jnp.arange(ep_count)[None, :]).astype(F32)
    earlier = (jnp.arange(pair_count)[:, None] > jnp.arange(pair_count)[None, :]).astype(F32)
    slots = jnp.sum(jnp.dot(earlier, onehot) * onehot, axis=1).astype(jnp.int32)
    target = (expert_ids * capacity + slots).reshape(seqs, topk)
    place = target[:, :, None] == jnp.arange(ep_count * capacity)[None, None, :]
    scaled = route_weight / jnp.sum(route_weight, axis=1, keepdims=True) * ROUTED_SCALE
    dispatch = jnp.any(place, axis=1).astype(BF)
    combine = jnp.sum(jnp.where(place, scaled[:, :, None], 0.0), axis=1)
    combine_high = combine.astype(BF)
    combine_low = (combine - combine_high.astype(F32)).astype(BF)

    residual, ffn_in, outgoing = call(
        post_kernel,
        [((seqs, width), BF), ((seqs, width), BF), ((ep_count, capacity, width), BF)],
        (*total_over_x(partial_mix), tokens, ffn_gain.reshape(1, width), dispatch),
        1 << 24,
    )
    received = exchange(outgoing, ("z", "y", "c")).reshape(-1, width)

    gate_up = jnp.concatenate((expert_gate[0], expert_up[0]), axis=1)
    (partial_rows,) = call(
        expert_kernel,
        [((ep_count, capacity, width), BF)],
        (received, gate_up, expert_down[0]),
        1 << 28,
    )
    returned = exchange(partial_rows, ("z", "y", "c"))
    returned = returned.reshape(-1, width)

    shared_own, shared_other = around_y_and_c(shared_block)
    (shared_part,) = call(
        shared_kernel,
        [((seqs, width), F32)],
        (ffn_in, branch_gate.reshape(1, width), shared_own, shared_other),
        1 << 25,
    )

    moe = dot(jnp.concatenate((combine_high, combine_low), axis=0), returned)
    addend = (moe[:seqs] + moe[seqs:] + shared_part).astype(BF)
    (layer_out,) = call(
        final_kernel, [((seqs, width), BF)], (*total_over_x(addend), residual), 1 << 20
    )
    return (layer_out, new_state)


def solution(mesh):
    ep, tp = mesh.devices.shape
    fine = Mesh(mesh.devices.reshape(ep // 8, 4, 2, tp), ("z", "y", "c", "x"))
    E = ("z", "y", "c")
    return jax.shard_map(
        per_device,
        mesh=fine,
        in_specs=(
            P(E, None),
            P(),
            P(E, "x"),
            P(E, "x"),
            P(E, "x"),
            P(E, "x"),
            P(),
            P(),
            P("x"),
            P("x"),
            P(),
            P(E, "x", None, None),
            P("x", E),
            P(),
            P(E, None),
            P(E, None),
            P(E, None, "x"),
            P(E, None, "x"),
            P(E, "x", None),
            P(E, "x"),
            P(E, "x"),
            P("x", E),
            P(),
        ),
        out_specs=(P(E, None), P(E, "x", None, None)),
        check_vma=False,
    )
```

```python
import functools

import jax
import jax.numpy as jnp
from jax import lax
from jax.experimental import pallas as pl
from jax.experimental.pallas import tpu as pltpu
from jax.sharding import Mesh
from jax.sharding import PartitionSpec as P

EPS = 1e-06
ROUTED_SCALE = 2.5
BF = jnp.bfloat16
F32 = jnp.float32
VMEM = pl.BlockSpec(memory_space=pltpu.VMEM)
HBM = pl.BlockSpec(memory_space=pltpu.HBM)
NT = (((1,), (1,)), ((), ()))


def rms_scale(values, gain):
    values = values.astype(F32)
    return (
        values
        * lax.rsqrt(jnp.mean(values * values, axis=-1, keepdims=True) + EPS)
        * gain.astype(F32)
    )


def unit_rows(values):
    return values * lax.rsqrt(jnp.sum(values * values, axis=-1, keepdims=True) + EPS)


def exchange(pieces, axis):
    return lax.all_to_all(pieces, axis, split_axis=0, concat_axis=0, tiled=True)


def dot(a, b):
    return jnp.dot(a, b, preferred_element_type=F32)


def shifted(array, axis, by):
    n = lax.axis_size(axis)
    return lax.ppermute(array, axis, [(i, (i + by) % n) for i in range(n)])


def around_y(block, cut):
    below = shifted(block, "y", 1)
    above = shifted(block, "y", -1)
    far_low = shifted(below[:cut], "y", 1)
    far_high = shifted(above[cut:], "y", -1)
    return block, below, (far_low, far_high), above


def around_y_and_c(block):
    below = shifted(block, "y", 1)
    above = shifted(block, "y", -1)
    far = shifted(below, "y", 1)
    own = jnp.stack((block, below, far, above))
    return own, shifted(own, "c", 1)


def total_over_x(part):
    return [part] + [shifted(part, "x", i) for i in (2, 1, 3)]


def four(a_ref, b_ref, c_ref, d_ref):
    a, b, c, d = (r[...].astype(F32) for r in (a_ref, b_ref, c_ref, d_ref))
    return (a + b) + (c + d)


def block_of(refs, z, y, c):
    near_ref, other_near_ref, *fars = refs
    at = lax.rem(lax.axis_index("y") - y + 4, 4)
    near = jnp.minimum(at, 2)
    mine = lax.axis_index("c") == c
    here = jnp.where(mine, near_ref[near, z], other_near_ref[near, z])
    half = fars[0].shape[0]
    far = jnp.where(mine, fars[z // half][z % half], fars[2 + z // half][z % half])
    return jnp.where(at == 2, far, here)


def group_rows(refs, group):
    z, first_y = group // 2, 2 * (group % 2)
    return jnp.concatenate(
        [block_of(refs, z, first_y + i // 2, i % 2) for i in range(4)], axis=0
    )


def prep_kernel(*refs):
    sources, (out_ref, normed_ref, weights_ref), targets = refs[:10], refs[10:13], list(refs[13:19])
    tok_ref, gain_ref, wo_ref, gate_ref, up_ref, down_ref = targets
    at = 0
    for source in sources[6:]:
        targets.append(weights_ref.at[:, at : at + source.shape[1]])
        at += source.shape[1]
    moves = [
        pltpu.make_async_copy(source, target, refs[19].at[i])
        for i, (source, target) in enumerate(zip(sources, targets))
    ]
    for move in moves:
        move.start()
    for move in moves[:6]:
        move.wait()
    half = tok_ref.shape[0] // 2
    values = tok_ref[...].astype(F32)
    scale = lax.rsqrt(jnp.mean(values * values, axis=-1, keepdims=True) + EPS)
    gain = gain_ref[...].astype(F32)
    peers, _, wide = out_ref.shape
    cols = wide // 2
    rows, hidden = gate_ref.shape
    for j in range(gain.shape[0]):
        lanes = slice(j * 128, (j + 1) * 128)
        part = (values[:, lanes] * scale * gain[j : j + 1]).astype(BF)
        normed_ref[:, lanes] = part
        z, at = j * 128 // cols, j * 128 % cols
        out_ref[z, 0:half, at : at + 128] = part[:half]
        out_ref[z, 0:half, cols + at : cols + at + 128] = part[half:]
    for z in range(peers):
        at = half
        out_ref[z, at : at + rows, :] = wo_ref[...]
        at += rows
        for i in range(2):
            part = slice(i * rows // 2, (i + 1) * rows // 2)
            out_ref[z, at : at + rows // 2, 2 * i * hidden : (2 * i + 1) * hidden] = gate_ref[part]
            out_ref[z, at : at + rows // 2, (2 * i + 1) * hidden : (2 * i + 2) * hidden] = up_ref[part]
        at += rows // 2
        for i in range(4):
            part = slice(i * rows // 4, (i + 1) * rows // 4)
            out_ref[z, at : at + rows // 4, i * hidden : (i + 1) * hidden] = down_ref[part]
    for move in moves[6:]:
        move.wait()


def proj_kernel(arr_ref, own_ref, other_ref, out_ref):
    peers, seqs, _ = out_ref.shape
    half = seqs // 2
    cols = arr_ref.shape[2] // 2
    parts = []
    for z in range(peers):
        parts += [arr_ref[z, 0:half, 0:cols], arr_ref[z, 0:half, cols : 2 * cols]]
    rows = jnp.concatenate(parts, axis=0)
    me_y, me_c = lax.axis_index("y"), lax.axis_index("c")
    blocks = []
    for i in range(8):
        at = lax.rem(me_y - i // 2 + 4, 4)
        blocks.append(jnp.where(me_c == i % 2, own_ref[at], other_ref[at]))
    part = dot(rows, jnp.concatenate(blocks, axis=0)).astype(BF)
    for z in range(peers):
        out_ref[z] = part[z * seqs : (z + 1) * seqs]


def state_copies(state_hbm, state_ref, sems):
    return [
        pltpu.make_async_copy(state_hbm.at[s], state_ref.at[s], sems.at[s])
        for s in range(state_ref.shape[0])
    ]


def delta_kernel(
    key_local, arr_ref, strength_ref, retain_ref, gain_ref, first_ref, state_hbm, heads_ref, fix_ref,
    keys_ref, state_ref, read_ref, sems,
):
    seqs, heads, key_dim, value_dim = state_ref.shape
    early = first_ref.shape[0]
    ins = state_copies(state_hbm, state_ref, sems)
    for copy in ins[early:]:
        copy.start()
    nq, nv = key_local * key_dim, heads * value_dim
    proj = jnp.sum(arr_ref[...].astype(F32), axis=0).astype(BF).astype(F32)
    silu = proj / (1.0 + jnp.exp(-proj))
    queries, keys, both = [], [], []
    for i in range(key_local):
        q = unit_rows(silu[:, i * key_dim : (i + 1) * key_dim]) * key_dim**-0.5
        k = unit_rows(silu[:, nq + i * key_dim : nq + (i + 1) * key_dim])
        both.append(jnp.sum(q * k, axis=1, keepdims=True))
        queries.append(q.T)
        keys.append(k.T)
        keys_ref[i] = k.T
    strength, retain = strength_ref[...], retain_ref[...]
    for s in range(seqs):
        if s >= early:
            ins[s].wait()
        for h in range(heads):
            i = h * key_local // heads
            if h * key_local % heads == 0:
                key = jnp.broadcast_to(keys[i][:, s : s + 1], (key_dim, value_dim))
                query = jnp.broadcast_to(queries[i][:, s : s + 1], (key_dim, value_dim))
            row = (slice(s, s + 1), slice(h, h + 1))
            state = first_ref[s, h] if s < early else state_ref[s, h]
            predicted = jnp.sum(state * key, axis=0, keepdims=True)
            asked = jnp.sum(state * query, axis=0, keepdims=True)
            at = 2 * nq + h * value_dim
            value = silu[s : s + 1, at : at + value_dim]
            correction = strength[row] * (value - retain[row] * predicted)
            cols = slice(h * value_dim, (h + 1) * value_dim)
            fix_ref[s : s + 1, cols] = correction
            read_ref[s : s + 1, cols] = retain[row] * asked + both[i][s : s + 1] * correction
    for h in range(heads):
        cols = slice(h * value_dim, (h + 1) * value_dim)
        gate = silu[:, 2 * nq + nv + h * value_dim : 2 * nq + nv + (h + 1) * value_dim]
        heads_ref[:, cols] = (rms_scale(read_ref[:, cols], gain_ref[...]) * gate).astype(BF)


def state_kernel(retain_ref, fix_ref, keys_ref, state_hbm, new_hbm, state_ref, new_ref, in_sems, sems):
    seqs, heads, _, value_dim = state_ref.shape
    ins = state_copies(state_hbm, state_ref, in_sems)
    for copy in ins:
        copy.start()
    retain = retain_ref[...]
    outs = []
    for s in range(seqs):
        ins[s].wait()
        for h in range(heads):
            kc = keys_ref[h * keys_ref.shape[0] // heads][:, s : s + 1]
            fix = fix_ref[s : s + 1, h * value_dim : (h + 1) * value_dim]
            new_ref[s, h] = state_ref[s, h] * retain[s : s + 1, h : h + 1] + kc * fix
        out = pltpu.make_async_copy(new_ref.at[s], new_hbm.at[s], sems.at[s])
        out.start()
        outs.append(out)
    for out in outs:
        out.wait()


def mix_kernel(heads_ref, *refs):
    heads, out_ref = heads_ref[...], refs[6]
    for group in range(out_ref.shape[1] // 128):
        rows = group_rows(refs[:6], group)
        part = lax.dot_general(heads, rows, NT, preferred_element_type=F32)
        out_ref[:, group * 128 : (group + 1) * 128] = part.astype(BF)


def post_kernel(a_ref, b_ref, c_ref, d_ref, tok_ref, gain_ref, dispatch_ref, res_ref, ffn_ref, out_ref):
    residual = (tok_ref[...].astype(F32) + four(a_ref, b_ref, c_ref, d_ref)).astype(BF)
    res_ref[...] = residual
    ffn_in = rms_scale(residual, gain_ref[...]).astype(BF)
    ffn_ref[...] = ffn_in
    out_ref[...] = lax.dot_general(
        dispatch_ref[...], ffn_in, (((0,), (0,)), ((), ())), preferred_element_type=F32
    ).astype(BF).reshape(out_ref.shape)


def final_kernel(a_ref, b_ref, c_ref, d_ref, res_ref, out_ref):
    out_ref[...] = (res_ref[...].astype(F32) + four(a_ref, b_ref, c_ref, d_ref)).astype(BF)


def shared_kernel(rows_ref, branch_ref, own_ref, other_ref, out_ref):
    groups = out_ref.shape[1] // 128
    hidden = own_ref.shape[3] // 4
    rows = rows_ref[...]
    total = jnp.zeros((rows.shape[0], 2 * hidden), F32)
    downs = []
    for group in range(groups):
        z, first_y = group // 2, 2 * (group % 2)
        block, down = [], []
        for i in range(4):
            at_y = lax.rem(lax.axis_index("y") - first_y - i // 2 + 4, 4)
            mine = lax.axis_index("c") == i % 2
            piece = jnp.where(mine, own_ref[at_y, z], other_ref[at_y, z])
            half = piece.shape[0] * 2 // 3
            block += [piece[:half, : 2 * hidden], piece[:half, 2 * hidden :]]
            down += [piece[half:, j * hidden : (j + 1) * hidden] for j in range(4)]
        downs.append(jnp.concatenate(down, axis=0))
        total += dot(rows[:, group * 128 : (group + 1) * 128], jnp.concatenate(block, axis=0))
    gate, up = total[:, :hidden], total[:, hidden:]
    act = (gate / (1.0 + jnp.exp(-gate)) * up).astype(BF)
    logit = jnp.sum(rows.astype(F32) * branch_ref[...].astype(F32), axis=1, keepdims=True)
    branch = 1.0 / (1.0 + jnp.exp(-logit))
    for group in range(groups):
        part = lax.dot_general(act, downs[group], NT, preferred_element_type=F32)
        out_ref[:, group * 128 : (group + 1) * 128] = branch * part


def expert_kernel(rows_ref, gate_up_ref, down_ref, out_ref):
    both = dot(rows_ref[...], gate_up_ref[...])
    hidden = both.shape[1] // 2
    gate, up = both[:, :hidden], both[:, hidden:]
    act = (gate / (1.0 + jnp.exp(-gate)) * up).astype(BF)
    out_ref[...] = dot(act, down_ref[...]).astype(BF).reshape(out_ref.shape)


def call(kernel, outs, args, flops, in_specs=None, out_specs=None, scratch=(), limit=16):
    moved = sum(a.size * a.dtype.itemsize for a in args)
    shapes = [jax.ShapeDtypeStruct(shape, dtype) for shape, dtype in outs]
    return pl.pallas_call(
        kernel,
        out_shape=shapes,
        in_specs=in_specs or [VMEM] * len(args),
        out_specs=out_specs or [VMEM] * len(shapes),
        scratch_shapes=list(scratch),
        cost_estimate=pl.CostEstimate(flops=flops, bytes_accessed=moved, transcendentals=0),
        compiler_params=pltpu.CompilerParams(vmem_limit_bytes=limit << 20),
    )(*args)


def per_device(
    tokens,
    norm_gain,
    query_weight,
    key_weight,
    value_weight,
    outgate_weight,
    beta_weight,
    decay_weight,
    decay_rate,
    decay_bias,
    head_gain,
    recurrent,
    output_weight,
    ffn_gain,
    routes,
    route_weight,
    expert_gate,
    expert_up,
    expert_down,
    shared_gate,
    shared_up,
    shared_down,
    branch_gate,
):
    nz, ny, nc, _ = (lax.axis_size(a) for a in "zycx")
    ep_count = nz * ny * nc
    seqs, width = tokens.shape
    heads, key_dim, value_dim = recurrent.shape[1:]
    block_k = width // nz
    inner = heads * value_dim

    wo_rows = output_weight.T
    half, rows = seqs // 2, wo_rows.shape[0]
    depth = half + rows + rows // 2 + rows // 4
    pieces = (query_weight, key_weight, value_weight, outgate_weight)
    across = sum(w.shape[1] for w in pieces)
    inputs = (tokens, norm_gain.reshape(width // 128, 128), wo_rows, shared_gate, shared_up, shared_down.T)
    packed, normed, weights = call(
        prep_kernel,
        [((nz, depth, 2 * block_k), BF), ((seqs, width), BF), ((rows, across), BF)],
        inputs + pieces,
        1 << 20,
        in_specs=[HBM] * 10,
        limit=60,
        scratch=[pltpu.VMEM(a.shape, BF) for a in inputs] + [pltpu.SemaphoreType.DMA((10,))],
    )
    arrived = exchange(packed, "z")
    wo_block = arrived[:, half : half + rows]
    shared_block = arrived[:, half + rows :]

    w_own, w_other = around_y_and_c(weights)

    (partial,) = call(
        proj_kernel, [((nz, seqs, weights.shape[1]), BF)], (arrived, w_own, w_other), 1 << 26
    )
    sums = exchange(partial, "z")

    wo_here, wo_below, wo_far, wo_above = around_y(wo_block, nz // 2)
    wo_near = jnp.stack((wo_here, wo_below, wo_above))
    wo_other_near = shifted(wo_near, "c", 1)
    wo_other_far = [shifted(half, "c", 1) for half in wo_far]

    head_start = lax.axis_index("x") * heads
    beta_logit = dot(normed, lax.dynamic_slice_in_dim(beta_weight, head_start, heads, 1))
    decay_logit = dot(normed, lax.dynamic_slice_in_dim(decay_weight, head_start, heads, 1))
    strength = jax.nn.sigmoid(beta_logit)
    retain = jnp.exp(-decay_rate[None, :] * jax.nn.softplus(decay_logit + decay_bias[None, :]))

    key_local = query_weight.shape[1] // key_dim
    first = recurrent[:2]
    heads_out, fixes, keys = call(
        functools.partial(delta_kernel, key_local),
        [((seqs, inner), BF), ((seqs, inner), F32), ((key_local, key_dim, seqs), F32)],
        (sums, strength, retain, head_gain.reshape(1, value_dim), first, recurrent),
        1 << 26,
        in_specs=[VMEM, VMEM, VMEM, VMEM, VMEM, HBM],
        limit=52,
        scratch=[
            pltpu.VMEM(recurrent.shape, F32),
            pltpu.VMEM((seqs, inner), F32),
            pltpu.SemaphoreType.DMA((seqs,)),
        ],
    )
    (new_state,) = call(
        state_kernel,
        [(recurrent.shape, F32)],
        (retain, fixes, keys, recurrent),
        1 << 26,
        in_specs=[VMEM, VMEM, VMEM, HBM],
        out_specs=[HBM],
        limit=52,
        scratch=[
            pltpu.VMEM(recurrent.shape, F32),
            pltpu.VMEM(recurrent.shape, F32),
            pltpu.SemaphoreType.DMA((seqs,)),
            pltpu.SemaphoreType.DMA((seqs,)),
        ],
    )
    (partial_mix,) = call(
        mix_kernel,
        [((seqs, width), BF)],
        (heads_out, wo_near, wo_other_near, *wo_far, *wo_other_far),
        1 << 25,
    )

    topk = routes.shape[1]
    pair_count = seqs * topk
    capacity = 2 * ((pair_count + ep_count - 1) // ep_count)
    expert_ids = routes.reshape(pair_count)
    onehot = (expert_ids[:, None] == jnp.arange(ep_count)[None, :]).astype(F32)
    earlier = (jnp.arange(pair_count)[:, None] > jnp.arange(pair_count)[None, :]).astype(F32)
    slots = jnp.sum(jnp.dot(earlier, onehot) * onehot, axis=1).astype(jnp.int32)
    target = (expert_ids * capacity + slots).reshape(seqs, topk)
    place = target[:, :, None] == jnp.arange(ep_count * capacity)[None, None, :]
    scaled = route_weight / jnp.sum(route_weight, axis=1, keepdims=True) * ROUTED_SCALE
    dispatch = jnp.any(place, axis=1).astype(BF)
    combine = jnp.sum(jnp.where(place, scaled[:, :, None], 0.0), axis=1)
    combine_high = combine.astype(BF)
    combine_low = (combine - combine_high.astype(F32)).astype(BF)

    residual, ffn_in, outgoing = call(
        post_kernel,
        [((seqs, width), BF), ((seqs, width), BF), ((ep_count, capacity, width), BF)],
        (*total_over_x(partial_mix), tokens, ffn_gain.reshape(1, width), dispatch),
        1 << 24,
    )
    received = exchange(outgoing, ("z", "y", "c")).reshape(-1, width)

    gate_up = jnp.concatenate((expert_gate[0], expert_up[0]), axis=1)
    (partial_rows,) = call(
        expert_kernel,
        [((ep_count, capacity, width), BF)],
        (received, gate_up, expert_down[0]),
        1 << 28,
    )
    returned = exchange(partial_rows, ("z", "y", "c"))
    returned = returned.reshape(-1, width)

    shared_own, shared_other = around_y_and_c(shared_block)
    (shared_part,) = call(
        shared_kernel,
        [((seqs, width), F32)],
        (ffn_in, branch_gate.reshape(1, width), shared_own, shared_other),
        1 << 25,
    )

    moe = dot(jnp.concatenate((combine_high, combine_low), axis=0), returned)
    addend = (moe[:seqs] + moe[seqs:] + shared_part).astype(BF)
    (layer_out,) = call(
        final_kernel, [((seqs, width), BF)], (*total_over_x(addend), residual), 1 << 20
    )
    return (layer_out, new_state)


def solution(mesh):
    ep, tp = mesh.devices.shape
    fine = Mesh(mesh.devices.reshape(ep // 8, 4, 2, tp), ("z", "y", "c", "x"))
    E = ("z", "y", "c")
    return jax.shard_map(
        per_device,
        mesh=fine,
        in_specs=(
            P(E, None),
            P(),
            P(E, "x"),
            P(E, "x"),
            P(E, "x"),
            P(E, "x"),
            P(),
            P(),
            P("x"),
            P("x"),
            P(),
            P(E, "x", None, None),
            P("x", E),
            P(),
            P(E, None),
            P(E, None),
            P(E, None, "x"),
            P(E, None, "x"),
            P(E, "x", None),
            P(E, "x"),
            P(E, "x"),
            P("x", E),
            P(),
        ),
        out_specs=(P(E, None), P(E, "x", None, None)),
        check_vma=False,
    )
```

```python
import functools

import jax
import jax.numpy as jnp
from jax import lax
from jax.experimental import pallas as pl
from jax.experimental.pallas import tpu as pltpu
from jax.sharding import Mesh
from jax.sharding import PartitionSpec as P

EPS = 1e-06
ROUTED_SCALE = 2.5
BF = jnp.bfloat16
F32 = jnp.float32
VMEM = pl.BlockSpec(memory_space=pltpu.VMEM)
HBM = pl.BlockSpec(memory_space=pltpu.HBM)
NT = (((1,), (1,)), ((), ()))


def rms_scale(values, gain):
    values = values.astype(F32)
    return (
        values
        * lax.rsqrt(jnp.mean(values * values, axis=-1, keepdims=True) + EPS)
        * gain.astype(F32)
    )


def unit_rows(values):
    return values * lax.rsqrt(jnp.sum(values * values, axis=-1, keepdims=True) + EPS)


def exchange(pieces, axis):
    return lax.all_to_all(pieces, axis, split_axis=0, concat_axis=0, tiled=True)


def dot(a, b):
    return jnp.dot(a, b, preferred_element_type=F32)


def shifted(array, axis, by):
    n = lax.axis_size(axis)
    return lax.ppermute(array, axis, [(i, (i + by) % n) for i in range(n)])


def around_y(block, cut):
    below = shifted(block, "y", 1)
    above = shifted(block, "y", -1)
    far_low = shifted(below[:cut], "y", 1)
    far_high = shifted(above[cut:], "y", -1)
    return block, below, (far_low, far_high), above


def around_y_and_c(block):
    below = shifted(block, "y", 1)
    above = shifted(block, "y", -1)
    far = shifted(below, "y", 1)
    own = jnp.stack((block, below, far, above))
    return own, shifted(own, "c", 1)


def total_over_x(part):
    return [part] + [shifted(part, "x", i) for i in (2, 1, 3)]


def four(a_ref, b_ref, c_ref, d_ref):
    a, b, c, d = (r[...].astype(F32) for r in (a_ref, b_ref, c_ref, d_ref))
    return (a + b) + (c + d)


def block_of(refs, z, y, c):
    near_ref, other_near_ref, *fars = refs
    at = lax.rem(lax.axis_index("y") - y + 4, 4)
    near = jnp.minimum(at, 2)
    mine = lax.axis_index("c") == c
    here = jnp.where(mine, near_ref[near, z], other_near_ref[near, z])
    half = fars[0].shape[0]
    far = jnp.where(mine, fars[z // half][z % half], fars[2 + z // half][z % half])
    return jnp.where(at == 2, far, here)


def group_rows(refs, group):
    z, first_y = group // 2, 2 * (group % 2)
    return jnp.concatenate(
        [block_of(refs, z, first_y + i // 2, i % 2) for i in range(4)], axis=0
    )


def prep_kernel(*refs):
    sources, (out_ref, normed_ref, weights_ref), targets = refs[:10], refs[10:13], list(refs[13:19])
    tok_ref, gain_ref, wo_ref, gate_ref, up_ref, down_ref = targets
    at = 0
    for source in sources[6:]:
        targets.append(weights_ref.at[:, at : at + source.shape[1]])
        at += source.shape[1]
    moves = [
        pltpu.make_async_copy(source, target, refs[19].at[i])
        for i, (source, target) in enumerate(zip(sources, targets))
    ]
    for move in moves:
        move.start()
    for move in moves[:6]:
        move.wait()
    half = tok_ref.shape[0] // 2
    values = tok_ref[...].astype(F32)
    scale = lax.rsqrt(jnp.mean(values * values, axis=-1, keepdims=True) + EPS)
    gain = gain_ref[...].astype(F32)
    peers, _, wide = out_ref.shape
    cols = wide // 2
    rows, hidden = gate_ref.shape
    for j in range(gain.shape[0]):
        lanes = slice(j * 128, (j + 1) * 128)
        part = (values[:, lanes] * scale * gain[j : j + 1]).astype(BF)
        normed_ref[:, lanes] = part
        z, at = j * 128 // cols, j * 128 % cols
        out_ref[z, 0:half, at : at + 128] = part[:half]
        out_ref[z, 0:half, cols + at : cols + at + 128] = part[half:]
    for z in range(peers):
        at = half
        out_ref[z, at : at + rows, :] = wo_ref[...]
        at += rows
        for i in range(2):
            part = slice(i * rows // 2, (i + 1) * rows // 2)
            out_ref[z, at : at + rows // 2, 2 * i * hidden : (2 * i + 1) * hidden] = gate_ref[part]
            out_ref[z, at : at + rows // 2, (2 * i + 1) * hidden : (2 * i + 2) * hidden] = up_ref[part]
        at += rows // 2
        for i in range(4):
            part = slice(i * rows // 4, (i + 1) * rows // 4)
            out_ref[z, at : at + rows // 4, i * hidden : (i + 1) * hidden] = down_ref[part]
    for move in moves[6:]:
        move.wait()


def proj_kernel(arr_ref, own_ref, other_ref, out_ref):
    peers, seqs, _ = out_ref.shape
    half = seqs // 2
    cols = arr_ref.shape[2] // 2
    parts = []
    for z in range(peers):
        parts += [arr_ref[z, 0:half, 0:cols], arr_ref[z, 0:half, cols : 2 * cols]]
    rows = jnp.concatenate(parts, axis=0)
    me_y, me_c = lax.axis_index("y"), lax.axis_index("c")
    blocks = []
    for i in range(8):
        at = lax.rem(me_y - i // 2 + 4, 4)
        blocks.append(jnp.where(me_c == i % 2, own_ref[at], other_ref[at]))
    part = dot(rows, jnp.concatenate(blocks, axis=0)).astype(BF)
    for z in range(peers):
        out_ref[z] = part[z * seqs : (z + 1) * seqs]


def state_copies(state_hbm, state_ref, sems):
    return [
        pltpu.make_async_copy(state_hbm.at[s], state_ref.at[s], sems.at[s])
        for s in range(state_ref.shape[0])
    ]


def delta_kernel(
    key_local, arr_ref, strength_ref, retain_ref, gain_ref, state_hbm, heads_ref, fix_ref, keys_ref,
    state_ref, read_ref, sems,
):
    seqs, heads, key_dim, value_dim = state_ref.shape
    ins = state_copies(state_hbm, state_ref, sems)
    for copy in ins[:3]:
        copy.start()
    nq, nv = key_local * key_dim, heads * value_dim
    proj = jnp.sum(arr_ref[...].astype(F32), axis=0).astype(BF).astype(F32)
    silu = proj / (1.0 + jnp.exp(-proj))
    queries, keys, both = [], [], []
    for i in range(key_local):
        q = unit_rows(silu[:, i * key_dim : (i + 1) * key_dim]) * key_dim**-0.5
        k = unit_rows(silu[:, nq + i * key_dim : nq + (i + 1) * key_dim])
        both.append(jnp.sum(q * k, axis=1, keepdims=True))
        queries.append(q.T)
        keys.append(k.T)
        keys_ref[i] = k.T
    strength, retain = strength_ref[...], retain_ref[...]
    for copy in ins[3:]:
        copy.start()
    for s in range(seqs):
        ins[s].wait()
        for h in range(heads):
            i = h * key_local // heads
            row = (slice(s, s + 1), slice(h, h + 1))
            if h * key_local % heads == 0:
                key = jnp.broadcast_to(keys[i][:, s : s + 1], (key_dim, value_dim))
                query = jnp.broadcast_to(queries[i][:, s : s + 1], (key_dim, value_dim))
            state = state_ref[s, h]
            predicted = jnp.sum(state * key, axis=0, keepdims=True)
            asked = jnp.sum(state * query, axis=0, keepdims=True)
            at = 2 * nq + h * value_dim
            value = silu[s : s + 1, at : at + value_dim]
            correction = strength[row] * (value - retain[row] * predicted)
            cols = slice(h * value_dim, (h + 1) * value_dim)
            fix_ref[s : s + 1, cols] = correction
            read_ref[s : s + 1, cols] = retain[row] * asked + both[i][s : s + 1] * correction
    for h in range(heads):
        cols = slice(h * value_dim, (h + 1) * value_dim)
        gate = silu[:, 2 * nq + nv + h * value_dim : 2 * nq + nv + (h + 1) * value_dim]
        heads_ref[:, cols] = (rms_scale(read_ref[:, cols], gain_ref[...]) * gate).astype(BF)


def state_kernel(retain_ref, fix_ref, keys_ref, state_hbm, new_hbm, state_ref, new_ref, in_sems, sems):
    seqs, heads, _, value_dim = state_ref.shape
    ins = state_copies(state_hbm, state_ref, in_sems)
    for copy in ins:
        copy.start()
    retain = retain_ref[...]
    outs = []
    for s in range(seqs):
        ins[s].wait()
        for h in range(heads):
            kc = keys_ref[h * keys_ref.shape[0] // heads][:, s : s + 1]
            fix = fix_ref[s : s + 1, h * value_dim : (h + 1) * value_dim]
            new_ref[s, h] = state_ref[s, h] * retain[s : s + 1, h : h + 1] + kc * fix
        out = pltpu.make_async_copy(new_ref.at[s], new_hbm.at[s], sems.at[s])
        out.start()
        outs.append(out)
    for out in outs:
        out.wait()


def mix_kernel(heads_ref, *refs):
    heads, out_ref = heads_ref[...], refs[6]
    for group in range(out_ref.shape[1] // 128):
        rows = group_rows(refs[:6], group)
        part = lax.dot_general(heads, rows, NT, preferred_element_type=F32)
        out_ref[:, group * 128 : (group + 1) * 128] = part.astype(BF)


def post_kernel(a_ref, b_ref, c_ref, d_ref, tok_ref, gain_ref, dispatch_ref, res_ref, ffn_ref, out_ref):
    residual = (tok_ref[...].astype(F32) + four(a_ref, b_ref, c_ref, d_ref)).astype(BF)
    res_ref[...] = residual
    ffn_in = rms_scale(residual, gain_ref[...]).astype(BF)
    ffn_ref[...] = ffn_in
    out_ref[...] = lax.dot_general(
        dispatch_ref[...], ffn_in, (((0,), (0,)), ((), ())), preferred_element_type=F32
    ).astype(BF).reshape(out_ref.shape)


def final_kernel(a_ref, b_ref, c_ref, d_ref, res_ref, out_ref):
    out_ref[...] = (res_ref[...].astype(F32) + four(a_ref, b_ref, c_ref, d_ref)).astype(BF)


def shared_kernel(rows_ref, branch_ref, own_ref, other_ref, out_ref):
    groups = out_ref.shape[1] // 128
    hidden = own_ref.shape[3] // 4
    rows = rows_ref[...]
    total = jnp.zeros((rows.shape[0], 2 * hidden), F32)
    downs = []
    for group in range(groups):
        z, first_y = group // 2, 2 * (group % 2)
        block, down = [], []
        for i in range(4):
            at_y = lax.rem(lax.axis_index("y") - first_y - i // 2 + 4, 4)
            mine = lax.axis_index("c") == i % 2
            piece = jnp.where(mine, own_ref[at_y, z], other_ref[at_y, z])
            half = piece.shape[0] * 2 // 3
            block += [piece[:half, : 2 * hidden], piece[:half, 2 * hidden :]]
            down += [piece[half:, j * hidden : (j + 1) * hidden] for j in range(4)]
        downs.append(jnp.concatenate(down, axis=0))
        total += dot(rows[:, group * 128 : (group + 1) * 128], jnp.concatenate(block, axis=0))
    gate, up = total[:, :hidden], total[:, hidden:]
    act = (gate / (1.0 + jnp.exp(-gate)) * up).astype(BF)
    logit = jnp.sum(rows.astype(F32) * branch_ref[...].astype(F32), axis=1, keepdims=True)
    branch = 1.0 / (1.0 + jnp.exp(-logit))
    for group in range(groups):
        part = lax.dot_general(act, downs[group], NT, preferred_element_type=F32)
        out_ref[:, group * 128 : (group + 1) * 128] = branch * part


def expert_kernel(rows_ref, gate_up_ref, down_ref, out_ref):
    both = dot(rows_ref[...], gate_up_ref[...])
    hidden = both.shape[1] // 2
    gate, up = both[:, :hidden], both[:, hidden:]
    act = (gate / (1.0 + jnp.exp(-gate)) * up).astype(BF)
    out_ref[...] = dot(act, down_ref[...]).astype(BF).reshape(out_ref.shape)


def call(kernel, outs, args, flops, in_specs=None, out_specs=None, scratch=(), limit=16):
    moved = sum(a.size * a.dtype.itemsize for a in args)
    shapes = [jax.ShapeDtypeStruct(shape, dtype) for shape, dtype in outs]
    return pl.pallas_call(
        kernel,
        out_shape=shapes,
        in_specs=in_specs or [VMEM] * len(args),
        out_specs=out_specs or [VMEM] * len(shapes),
        scratch_shapes=list(scratch),
        cost_estimate=pl.CostEstimate(flops=flops, bytes_accessed=moved, transcendentals=0),
        compiler_params=pltpu.CompilerParams(vmem_limit_bytes=limit << 20),
    )(*args)


def per_device(
    tokens,
    norm_gain,
    query_weight,
    key_weight,
    value_weight,
    outgate_weight,
    beta_weight,
    decay_weight,
    decay_rate,
    decay_bias,
    head_gain,
    recurrent,
    output_weight,
    ffn_gain,
    routes,
    route_weight,
    expert_gate,
    expert_up,
    expert_down,
    shared_gate,
    shared_up,
    shared_down,
    branch_gate,
):
    nz, ny, nc, _ = (lax.axis_size(a) for a in "zycx")
    ep_count = nz * ny * nc
    seqs, width = tokens.shape
    heads, key_dim, value_dim = recurrent.shape[1:]
    block_k = width // nz
    inner = heads * value_dim

    wo_rows = output_weight.T
    half, rows = seqs // 2, wo_rows.shape[0]
    depth = half + rows + rows // 2 + rows // 4
    pieces = (query_weight, key_weight, value_weight, outgate_weight)
    across = sum(w.shape[1] for w in pieces)
    inputs = (tokens, norm_gain.reshape(width // 128, 128), wo_rows, shared_gate, shared_up, shared_down.T)
    packed, normed, weights = call(
        prep_kernel,
        [((nz, depth, 2 * block_k), BF), ((seqs, width), BF), ((rows, across), BF)],
        inputs + pieces,
        1 << 20,
        in_specs=[HBM] * 10,
        limit=60,
        scratch=[pltpu.VMEM(a.shape, BF) for a in inputs] + [pltpu.SemaphoreType.DMA((10,))],
    )
    arrived = exchange(packed, "z")
    wo_block = arrived[:, half : half + rows]
    shared_block = arrived[:, half + rows :]

    w_own, w_other = around_y_and_c(weights)

    (partial,) = call(
        proj_kernel, [((nz, seqs, weights.shape[1]), BF)], (arrived, w_own, w_other), 1 << 26
    )
    sums = exchange(partial, "z")

    wo_here, wo_below, wo_far, wo_above = around_y(wo_block, nz // 2)
    wo_near = jnp.stack((wo_here, wo_below, wo_above))
    wo_other_near = shifted(wo_near, "c", 1)
    wo_other_far = [shifted(half, "c", 1) for half in wo_far]

    head_start = lax.axis_index("x") * heads
    beta_logit = dot(normed, lax.dynamic_slice_in_dim(beta_weight, head_start, heads, 1))
    decay_logit = dot(normed, lax.dynamic_slice_in_dim(decay_weight, head_start, heads, 1))
    strength = jax.nn.sigmoid(beta_logit)
    retain = jnp.exp(-decay_rate[None, :] * jax.nn.softplus(decay_logit + decay_bias[None, :]))

    key_local = query_weight.shape[1] // key_dim
    heads_out, fixes, keys = call(
        functools.partial(delta_kernel, key_local),
        [((seqs, inner), BF), ((seqs, inner), F32), ((key_local, key_dim, seqs), F32)],
        (sums, strength, retain, head_gain.reshape(1, value_dim), recurrent),
        1 << 26,
        in_specs=[VMEM, VMEM, VMEM, VMEM, HBM],
        limit=52,
        scratch=[
            pltpu.VMEM(recurrent.shape, F32),
            pltpu.VMEM((seqs, inner), F32),
            pltpu.SemaphoreType.DMA((seqs,)),
        ],
    )
    (new_state,) = call(
        state_kernel,
        [(recurrent.shape, F32)],
        (retain, fixes, keys, recurrent),
        1 << 26,
        in_specs=[VMEM, VMEM, VMEM, HBM],
        out_specs=[HBM],
        limit=52,
        scratch=[
            pltpu.VMEM(recurrent.shape, F32),
            pltpu.VMEM(recurrent.shape, F32),
            pltpu.SemaphoreType.DMA((seqs,)),
            pltpu.SemaphoreType.DMA((seqs,)),
        ],
    )
    (partial_mix,) = call(
        mix_kernel,
        [((seqs, width), BF)],
        (heads_out, wo_near, wo_other_near, *wo_far, *wo_other_far),
        1 << 25,
    )

    topk = routes.shape[1]
    pair_count = seqs * topk
    capacity = 2 * ((pair_count + ep_count - 1) // ep_count)
    expert_ids = routes.reshape(pair_count)
    onehot = (expert_ids[:, None] == jnp.arange(ep_count)[None, :]).astype(F32)
    earlier = (jnp.arange(pair_count)[:, None] > jnp.arange(pair_count)[None, :]).astype(F32)
    slots = jnp.sum(jnp.dot(earlier, onehot) * onehot, axis=1).astype(jnp.int32)
    target = (expert_ids * capacity + slots).reshape(seqs, topk)
    place = target[:, :, None] == jnp.arange(ep_count * capacity)[None, None, :]
    scaled = route_weight / jnp.sum(route_weight, axis=1, keepdims=True) * ROUTED_SCALE
    dispatch = jnp.any(place, axis=1).astype(BF)
    combine = jnp.sum(jnp.where(place, scaled[:, :, None], 0.0), axis=1)
    combine_high = combine.astype(BF)
    combine_low = (combine - combine_high.astype(F32)).astype(BF)

    residual, ffn_in, outgoing = call(
        post_kernel,
        [((seqs, width), BF), ((seqs, width), BF), ((ep_count, capacity, width), BF)],
        (*total_over_x(partial_mix), tokens, ffn_gain.reshape(1, width), dispatch),
        1 << 24,
    )
    received = exchange(outgoing, ("z", "y", "c")).reshape(-1, width)

    gate_up = jnp.concatenate((expert_gate[0], expert_up[0]), axis=1)
    (partial_rows,) = call(
        expert_kernel,
        [((ep_count, capacity, width), BF)],
        (received, gate_up, expert_down[0]),
        1 << 28,
    )
    returned = exchange(partial_rows, ("z", "y", "c"))
    returned = returned.reshape(-1, width)

    shared_own, shared_other = around_y_and_c(shared_block)
    (shared_part,) = call(
        shared_kernel,
        [((seqs, width), F32)],
        (ffn_in, branch_gate.reshape(1, width), shared_own, shared_other),
        1 << 25,
    )

    moe = dot(jnp.concatenate((combine_high, combine_low), axis=0), returned)
    addend = (moe[:seqs] + moe[seqs:] + shared_part).astype(BF)
    (layer_out,) = call(
        final_kernel, [((seqs, width), BF)], (*total_over_x(addend), residual), 1 << 20
    )
    return (layer_out, new_state)


def solution(mesh):
    ep, tp = mesh.devices.shape
    fine = Mesh(mesh.devices.reshape(ep // 8, 4, 2, tp), ("z", "y", "c", "x"))
    E = ("z", "y", "c")
    return jax.shard_map(
        per_device,
        mesh=fine,
        in_specs=(
            P(E, None),
            P(),
            P(E, "x"),
            P(E, "x"),
            P(E, "x"),
            P(E, "x"),
            P(),
            P(),
            P("x"),
            P("x"),
            P(),
            P(E, "x", None, None),
            P("x", E),
            P(),
            P(E, None),
            P(E, None),
            P(E, None, "x"),
            P(E, None, "x"),
            P(E, "x", None),
            P(E, "x"),
            P(E, "x"),
            P("x", E),
            P(),
        ),
        out_specs=(P(E, None), P(E, "x", None, None)),
        check_vma=False,
    )
```
